512 devices in a mesh: sp: 16 (over z), dp: 32 (over y, x, core).
Axes of the slice: x: 4, y: 4, z: 16, core: 2. Of those that a mesh axis runs over, the one named last changes fastest.
Arguments:
- stream_x: bfloat16 [32, 2048, 2048], P('dp', 'sp'), may hold values from -6 to 6
- stream_b: bfloat16 [32, 2048, 1024], P('dp', 'sp'), may hold values from -6 to 6
- stream_c: bfloat16 [32, 2048, 1024], P('dp', 'sp'), may hold values from -6 to 6
- gate_z: bfloat16 [32, 2048, 2048], P('dp', 'sp'), may hold values from -6 to 6
- step_raw: bfloat16 [32, 2048, 32], P('dp', 'sp'), may hold values from -4 to 3
- conv_x: bfloat16 [4, 2048], P(None, 'sp'), may hold values from -3 to 3
- conv_b: bfloat16 [4, 1024], replicated, may hold values from -3 to 3
- conv_c: bfloat16 [4, 1024], replicated, may hold values from -3 to 3
- decay_log: float32 [32], P('sp'), may hold values from -20 to 0
- norm_gain: float32 [2048], replicated, may hold values from 0.1 to 1.9
- w_out: bfloat16 [2048, 2048], P('dp'), may hold values from -0.125 to 0.125
Outputs:
- mixed: bfloat16 [32, 2048, 2048], P('dp', 'sp')
The draws below stay inside these ranges and needn't reach their ends.
All inputs are finite; a program needn't handle non-finite values.
Results may differ from the reference program's by a relative error of at most 0.011.
Values may be sent and summed in bfloat16 or wider, within the bound.
A program may use at most 64 MiB of HBM per device.

```python
import jax
import jax.numpy as jnp
from jax import lax

D = 2048
HEADS = 32
HEAD_DIM = 64
STATE = 128
CONV = 4
BLOCK = 64
TOK_DEV = 128
DI = 2048
GROUP_STATE = 1024
SEQS = 32
LEN = 2048


def draw_step_raw(key, part):
    first_key, second_key = jax.random.split(jax.random.fold_in(key, 11))
    noise = jnp.clip(jax.random.normal(first_key, (SEQS, LEN, HEADS), jnp.float32), -3.0, 3.0)
    offset = jax.random.uniform(second_key, (SEQS, LEN // TOK_DEV, 1, HEADS), jnp.float32, -2.0, 1.0)
    offset = jnp.broadcast_to(offset, (SEQS, LEN // TOK_DEV, TOK_DEV, HEADS)).reshape(SEQS, LEN, HEADS)
    return (0.6 * noise + offset).astype(jnp.bfloat16)


def draw_decay_log(key, part):
    pick_key, slow_key, quick_key = jax.random.split(jax.random.fold_in(key, 23), 3)
    chance = 0.5
    quick_heads = jax.random.uniform(pick_key, (HEADS,), jnp.float32) < chance
    slow_rate = jax.random.uniform(slow_key, (HEADS,), jnp.float32, 0.3, 1.0) / LEN
    quick_rate = jax.random.uniform(quick_key, (HEADS,), jnp.float32, 0.03, 0.08)
    return jnp.log(jnp.where(quick_heads, quick_rate, slow_rate)).astype(jnp.float32)


def shard_levels(key, dims, cuts, least, largest):
    factor_of, own = 1.0, jax.random.fold_in(key, 6)
    for position, blocks in cuts:
        heights = jnp.exp(jax.random.uniform(jax.random.fold_in(own, position), (blocks,), jnp.float32, least / len(cuts), largest / len(cuts)))
        factor_of = factor_of * jnp.repeat(heights, dims[position] // blocks).reshape([-1 if axis == position else 1 for axis in range(len(dims))])
    return factor_of


def scatter_about(own_key, extent, scale, limit, shards=(), dtype=jnp.bfloat16):
    factor_of = shard_levels(own_key, extent, shards, -0.22, 0.18) if shards else 1.0
    drawn = jax.random.normal(own_key, extent, jnp.float32) * scale * factor_of
    return jnp.minimum(jnp.maximum(drawn, -limit), limit).astype(dtype)


def setup_inputs(seed: int = 0) -> dict:
    seeds = jax.random.split(jax.random.key(seed), 12)
    return {
        "stream_x": scatter_about(seeds[0], (SEQS, LEN, DI), 1.0, 6.0, ((0, 32), (1, 16))),
        "stream_b": scatter_about(seeds[1], (SEQS, LEN, GROUP_STATE), 1.0, 6.0, ((0, 32), (1, 16))),
        "stream_c": scatter_about(seeds[2], (SEQS, LEN, GROUP_STATE), 1.0, 6.0, ((0, 32), (1, 16))),
        "gate_z": scatter_about(seeds[3], (SEQS, LEN, DI), 1.0, 6.0, ((0, 32), (1, 16))),
        "step_raw": draw_step_raw(jax.random.fold_in(seeds[11], 71), 0),
        "conv_x": scatter_about(seeds[5], (CONV, DI), CONV ** -0.5, 3.0, ((1, 16),)),
        "conv_b": scatter_about(seeds[6], (CONV, GROUP_STATE), CONV ** -0.5, 3.0),
        "conv_c": scatter_about(seeds[7], (CONV, GROUP_STATE), CONV ** -0.5, 3.0),
        "decay_log": draw_decay_log(jax.random.fold_in(seeds[11], 71), 0),
        "norm_gain": jnp.clip(1.0 + 0.18 * jax.random.normal(seeds[9], (DI,), jnp.float32), 0.1, 1.9),
        "w_out": scatter_about(seeds[10], (DI, D), DI ** -0.5, 0.125, ((0, 32),)),
    }


NORM_EPS = 1.0

def causal_conv(sequence, kernel):
    taps = kernel.shape[0]
    length = sequence.shape[0]
    padded = jnp.pad(sequence.astype(jnp.float32), ((taps - 1, 0), (0, 0)))
    summed = jnp.zeros(sequence.shape, jnp.float32)
    for tap_index in range(taps):
        summed = summed + kernel[tap_index].astype(jnp.float32) * padded[tap_index:tap_index + length]
    rounded = lax.optimization_barrier(jax.nn.silu(summed).astype(jnp.bfloat16))
    return rounded.astype(jnp.float32)

def mixer(seq_x, seq_b, seq_c, seq_raw, conv_x, conv_b, conv_c, decay_log):
    length = seq_x.shape[0]
    head_count = seq_raw.shape[1]
    group_count = seq_b.shape[1] // STATE
    ratio = head_count // group_count
    blocks = length // BLOCK
    highest = lax.Precision.HIGHEST
    x_values = causal_conv(seq_x, conv_x).reshape(blocks, BLOCK, group_count, ratio, HEAD_DIM)
    b_values = causal_conv(seq_b, conv_b).reshape(blocks, BLOCK, group_count, STATE)
    c_values = causal_conv(seq_c, conv_c).reshape(blocks, BLOCK, group_count, STATE)
    step_size = jax.nn.softplus(seq_raw.astype(jnp.float32))
    log_decay = (step_size * (-jnp.exp(decay_log))[None, :]).reshape(blocks, BLOCK, group_count, ratio)
    step_size = step_size.reshape(blocks, BLOCK, group_count, ratio)
    cumul = jnp.cumsum(log_decay, axis=1)
    scores = jnp.einsum('kTgn,kSgn->kTSg', c_values, b_values, precision=highest)
    causal = jnp.tril(jnp.ones((BLOCK, BLOCK), bool))
    spread = cumul[:, :, None] - cumul[:, None, :]
    decay = jnp.exp(jnp.where(causal[None, :, :, None, None], spread, -jnp.inf))
    weights = scores[..., None] * decay * step_size[:, None]
    inner = jnp.einsum('kTSgr,kSgrp->kTgrp', weights, x_values, precision=highest)
    last = cumul[:, -1]
    tail = jnp.exp(last[:, None] - cumul) * step_size
    local = jnp.einsum('kSgn,kSgr,kSgrp->kgrpn', b_values, tail, x_values, precision=highest)
    before = jnp.cumsum(last, axis=0) - last
    after = before + last
    gap = before[:, None] - after[None, :]
    lower = jnp.tril(jnp.ones((blocks, blocks), bool), -1)
    carry_weight = jnp.exp(jnp.where(lower[:, :, None, None], gap, -jnp.inf))
    entering = jnp.einsum('kjgr,jgrpn->kgrpn', carry_weight, local, precision=highest)
    carried = jnp.einsum('kTgn,kgrpn,kTgr->kTgrp', c_values, entering, jnp.exp(cumul), precision=highest)
    return (inner + carried).reshape(length, head_count * HEAD_DIM).astype(jnp.bfloat16)

def gate_norm(core_out, seq_z, gain, group_width):
    length = core_out.shape[0]
    gated = core_out.astype(jnp.float32) * jax.nn.silu(seq_z.astype(jnp.float32))
    grouped = gated.reshape(length, -1, group_width)
    scale = lax.rsqrt(lax.optimization_barrier(jnp.mean(grouped * grouped, axis=-1, keepdims=True)) + NORM_EPS)
    return ((grouped * scale).reshape(length, -1) * gain[None, :]).astype(jnp.bfloat16)

def reference(stream_x, stream_b, stream_c, gate_z, step_raw, conv_x, conv_b, conv_c, decay_log, norm_gain, w_out):
    group_width = HEAD_DIM

    def one_sequence(inputs):
        seq_x, seq_b, seq_c, seq_z, seq_raw = inputs
        core_out = mixer(seq_x, seq_b, seq_c, seq_raw, conv_x, conv_b, conv_c, decay_log)
        normed = gate_norm(core_out, seq_z, norm_gain, group_width)
        return jnp.dot(normed, w_out, preferred_element_type=jnp.float32).astype(jnp.bfloat16)
    return lax.map(one_sequence, (stream_x, stream_b, stream_c, gate_z, step_raw))
```

```python
import functools
import math

import jax
import jax.numpy as jnp
from jax import lax
from jax.experimental import pallas as pl
from jax.experimental.pallas import tpu as pltpu
from jax.sharding import PartitionSpec as P

HEAD_DIM = 64
STATE = 128
NORM_EPS = 1.0
HALO = 16
LANES = 128
HOP = 2
RELAYS = (8, 11, 14, 18)
READY = 20
F32 = jnp.float32
BF16 = jnp.bfloat16


def dot(a, b, precision=None):
    return jnp.dot(a, b, preferred_element_type=F32, precision=precision)


def silu(v):
    return v / (1.0 + jnp.exp(-v))


def kernel(
    sp,
    dp,
    x_hbm,
    b_hbm,
    c_hbm,
    z_hbm,
    raw_ref,
    cx_hbm,
    cb_hbm,
    cc_hbm,
    dl_ref,
    gain_hbm,
    w_hbm,
    out_ref,
    cx_ref,
    cb_ref,
    cc_ref,
    gain_ref,
    x_v,
    b_v,
    c_v,
    z_v,
    halo_x,
    halo_b,
    halo_c,
    par,
    taps,
    wide_raw,
    ext,
    zs,
    scores,
    b_ts,
    xlow,
    inner,
    ecum,
    elast,
    wts,
    lasts,
    total,
    cact,
    local,
    a_in,
    a_out,
    b_in,
    b_out,
    normed,
    w_all,
    acc,
    in_sem,
    par_send,
    par_recv,
    last_send,
    last_recv,
    halo_send,
    halo_recv,
    a_send,
    a_recv,
    b_send,
    b_recv,
    own_sem,
    one_send,
    one_recv,
    two_send,
    two_recv,
    relay_send,
    relay_recv,
):
    tokens, inner_width = x_v.shape
    groups = b_v.shape[1] // STATE
    group_width = inner_width // groups
    pairs = group_width // LANES
    chunks = groups * pairs
    ratio = group_width // HEAD_DIM
    heads, local_heads = raw_ref.shape[1], dl_ref.shape[1]
    tap_count, tap_width = cx_ref.shape
    rows = w_hbm.shape[0]
    half_rows = rows // 2
    side = math.isqrt(dp // 2)
    cut = max(2, (3 * sp) // 8)
    middle = cut + (sp - cut + 1) // 2
    reach = max(cut, sp - cut) - 1

    pos = lax.axis_index("sp")
    me = lax.axis_index("dp")
    core = me % 2
    partner = me + 1 - 2 * core
    place = me // 2
    column, line = place % side, place // side
    following = (pos + 1) % sp
    preceding = (pos + sp - 1) % sp
    first = pos < cut

    def remote(src, dst, send, recv, target):
        return pltpu.make_async_remote_copy(
            src_ref=src,
            dst_ref=dst,
            send_sem=send,
            recv_sem=recv,
            device_id=target,
            device_id_type=pl.DeviceIdType.MESH,
        )

    def chip(axis, along, across):
        dx, dy = (along, across) if axis == 0 else (across, along)
        return ((line + dy + side) % side) * side + (column + dx + side) % side

    sources = (
        (cx_hbm, cx_ref),
        (b_hbm.at[0], b_v),
        (c_hbm.at[0], c_v),
        (x_hbm.at[0], x_v),
        (cb_hbm, cb_ref),
        (cc_hbm, cc_ref),
        (z_hbm.at[0], z_v),
        (gain_hbm, gain_ref),
    )
    loads = [
        pltpu.make_async_copy(src, dst, in_sem.at[i]) for i, (src, dst) in enumerate(sources)
    ]
    for load in loads:
        load.start()

    barrier = pltpu.get_barrier_semaphore()
    greeted = [{"sp": (pos + j) % sp} for j in range(1, sp)] + [{"dp": partner}]
    for axis in range(2):
        for i in range(1, side):
            greeted.append({"dp": 2 * chip(axis, i, 0) + core})
    for target in greeted:
        pl.semaphore_signal(
            barrier, inc=1, device_id=target, device_id_type=pl.DeviceIdType.MESH
        )

    def piece(axis, along, across):
        origin = 2 * chip(axis, along, across) + core
        start = pl.multiple_of(origin * rows + axis * half_rows, half_rows)
        return w_all.at[pl.ds(start, half_rows), :]

    own_rows = w_all.at[pl.ds(pl.multiple_of(me * rows, rows), rows), :]
    keep = pltpu.make_async_copy(w_hbm, own_rows, in_sem.at[len(sources)])
    keep.start()

    par[pos] = jnp.zeros(par.shape[1:], F32)
    wide_raw[...] = jnp.zeros(wide_raw.shape, F32)
    wide_raw[0:1, 0:local_heads] = dl_ref[...]
    par[pos, :, tap_width : tap_width + LANES] = pltpu.roll(
        wide_raw[0:8, :], pos * local_heads, 1
    )
    wide_raw[0:heads, :] = raw_ref[0].astype(F32)
    loads[0].wait()
    par[pos, 0:tap_count, 0:tap_width] = cx_ref[...].astype(F32)
    for load in loads[1:]:
        load.wait()
    keep.wait()
    pl.semaphore_wait(barrier, len(greeted))

    shares = [
        remote(
            par.at[pos],
            par.at[pos],
            par_send.at[j - 1],
            par_recv.at[j - 1],
            {"sp": (pos + j) % sp},
        )
        for j in range(1, sp)
    ]
    for copy in shares:
        copy.start()

    halos = [
        remote(
            src.at[pl.ds(tokens - HALO, HALO), :],
            dst,
            halo_send.at[i],
            halo_recv.at[i],
            {"sp": following},
        )
        for i, (src, dst) in enumerate(((x_v, halo_x), (b_v, halo_b), (c_v, halo_c)))
    ]

    @pl.when(pos < sp - 1)
    def _():
        for copy in halos:
            copy.start()

    def stage_one(axis, i):
        return remote(
            piece(axis, 0, 0),
            piece(axis, 0, 0),
            one_send.at[axis, i],
            one_recv.at[axis, i],
            {"dp": 2 * chip(axis, i, 0) + core},
        )

    def stage_two(axis, k, i):
        return remote(
            piece(axis, -k, 0),
            piece(axis, -k, 0),
            two_send.at[axis, k, i],
            two_recv.at[axis, k, i],
            {"dp": 2 * chip(axis, 0, i) + core},
        )

    def relay(axis, k, i):
        return remote(
            piece(axis, -k, -i),
            piece(axis, -k, -i),
            relay_send.at[axis, k, i],
            relay_recv.at[axis, k, i],
            {"dp": partner},
        )

    steps = sorted(range(1, side), key=lambda i: min(i, side - i))
    for i in steps:
        for axis in range(2):
            stage_one(axis, i).start()
    for i in steps:
        for axis in range(2):
            stage_two(axis, 0, i).start()
    own = remote(own_rows, own_rows, own_sem.at[0], own_sem.at[1], {"dp": partner})
    own.start()

    def spread_lines():
        for k in steps:
            for axis in range(2):
                stage_one(axis, k).wait_recv()
                for i in steps:
                    stage_two(axis, k, i).start()

    def pass_rows(step):
        if step == 0:
            for k in steps:
                for axis in range(2):
                    relay(axis, k, 0).start()
            which = 0
        else:
            which = steps[step - 1]
        for i in steps:
            for axis in range(2):
                stage_two(axis, which, i).wait_recv()
                relay(axis, which, i).start()

    raw = jnp.transpose(wide_raw[...])
    dt = jnp.maximum(raw, 0.0) + jnp.log(1.0 + jnp.exp(-jnp.abs(raw)))
    down = lax.broadcasted_iota(jnp.int32, (tokens, tokens), 0)
    across_tokens = lax.broadcasted_iota(jnp.int32, (tokens, tokens), 1)
    causal = down >= across_tokens
    left_half = lax.broadcasted_iota(jnp.int32, (tokens, LANES), 1) < HEAD_DIM
    left_row = left_half[0:1, :]
    for g in range(groups):
        taps[g, 0:tap_count, group_width : group_width + STATE] = cb_ref[
            :, g * STATE : (g + 1) * STATE
        ].astype(F32)
        taps[g, 0:tap_count, group_width + STATE : group_width + 2 * STATE] = cc_ref[
            :, g * STATE : (g + 1) * STATE
        ].astype(F32)
        zs[g] = silu(z_v[:, g * group_width : (g + 1) * group_width].astype(F32))

    @pl.when(pos == 0)
    def _():
        ext[:, 0:8, :] = jnp.zeros((groups, 8, ext.shape[2]), F32)

    @pl.when((pos == 0) | (pos == cut))
    def _():
        a_in[...] = jnp.zeros(a_in.shape, BF16)

    @pl.when(pos > 0)
    def _():
        for copy in halos:
            copy.wait_recv()
        for g in range(groups):
            wide = slice(g * group_width, (g + 1) * group_width)
            thin = slice(g * STATE, (g + 1) * STATE)
            ext[g, 0:8, 0:group_width] = halo_x[:, wide].astype(F32)[HALO - 8 :]
            ext[g, 0:8, group_width : group_width + STATE] = halo_b[:, thin].astype(F32)[
                HALO - 8 :
            ]
            ext[g, 0:8, group_width + STATE :] = halo_c[:, thin].astype(F32)[HALO - 8 :]

    def conv(g, source, at):
        columns = slice(at, at + LANES)
        ext[g, 8 : 8 + tokens, columns] = source.astype(F32)
        summed = taps[g, 0:1, columns] * ext[g, 9 - tap_count : 9 - tap_count + tokens, columns]
        for k in range(1, tap_count):
            start = 9 - tap_count + k
            summed = summed + taps[g, k : k + 1, columns] * ext[g, start : start + tokens, columns]
        return silu(summed).astype(BF16)

    for g in range(groups):
        thin = slice(g * STATE, (g + 1) * STATE)
        b_act = conv(g, b_v[:, thin], group_width)
        c_act = conv(g, c_v[:, thin], group_width + STATE)
        cact[g] = c_act
        b_t = jnp.transpose(b_act)
        b_ts[g] = b_t
        scores[g] = dot(c_act, b_t)

    for copy in shares:
        copy.wait_recv()
    rates = par[0, 0:1, tap_width : tap_width + LANES]
    for s in range(1, sp):
        rates = rates + par[s, 0:1, tap_width : tap_width + LANES]
    log_decay = dt * (-jnp.exp(rates))
    cum = dot(jnp.where(causal, 1.0, 0.0).astype(F32), log_decay, lax.Precision.HIGHEST)
    cum_t = jnp.transpose(cum)
    lasts[0] = jnp.broadcast_to(cum[tokens - 1 : tokens, :], lasts.shape[1:])

    def tell(d):
        target = jnp.where(first, pos + sp - d, pos + d) % sp
        return remote(
            lasts.at[0], lasts.at[d], last_send.at[d], last_recv.at[d], {"sp": target}
        )

    def tells(d):
        return (first & (pos >= d)) | (jnp.logical_not(first) & (pos + d < sp))

    def hears(d):
        return (first & (pos + d < cut)) | (jnp.logical_not(first) & (pos - d >= cut))

    for d in range(1, reach + 1):

        @pl.when(tells(d))
        def _():
            tell(d).start()

    for chunk in range(chunks):
        begin = chunk * LANES
        g, at = begin // group_width, begin % group_width
        s, off = begin // tap_width, begin % tap_width
        taps[g, 0:tap_count, at : at + LANES] = par[s, 0:tap_count, off : off + LANES]

    def chain(j):
        return remote(a_out.at[j], a_in.at[j], a_send.at[j], a_recv.at[j], {"sp": following})

    def cross(j):
        return remote(a_out.at[j], b_in.at[j], a_send.at[j], b_recv.at[j], {"sp": following})

    def back(j):
        return remote(b_out.at[j], b_in.at[j], b_send.at[j], b_recv.at[j], {"sp": preceding})

    def carry_up(j):
        return remote(b_in.at[j], b_in.at[j], b_send.at[j], b_recv.at[j], {"sp": following})

    def carry_down(j):
        return remote(b_in.at[j], b_in.at[j], b_send.at[j], b_recv.at[j], {"sp": preceding})

    carries_up = (pos >= cut) & (pos < middle - 1)
    carries_down = pos > middle

    for g in range(groups):
        b_t = b_ts[g]
        for p in range(pairs):
            j = g * pairs + p
            columns = slice(j * LANES, (j + 1) * LANES)
            local_columns = slice(p * LANES, (p + 1) * LANES)
            x_act = conv(g, x_v[:, columns], p * LANES).astype(F32)
            h = g * ratio + 2 * p
            step = jnp.where(left_half, dt[:, h : h + 1], dt[:, h + 1 : h + 2])
            both = jnp.where(left_half, cum[:, h : h + 1], cum[:, h + 1 : h + 2])
            x_dt = x_act * step
            xlow[g, :, local_columns] = x_dt.astype(BF16)
            ecum[g, :, local_columns] = jnp.exp(both)
            last = both[tokens - 1 : tokens, :]
            elast[j, 0:1, :] = jnp.exp(last)
            x_tail = (x_dt * jnp.exp(last - both)).astype(BF16)
            mine = dot(b_t, x_tail)
            local[j] = mine

            @pl.when((pos == 0) | (pos == cut))
            def _():
                a_out[j] = local[j].astype(BF16)
                chain(j).start()

            @pl.when(pos == cut - 1)
            def _():
                b_out[j] = local[j].astype(BF16)
                back(j).start()

    def weigh():
        total[...] = jnp.zeros(total.shape, F32)
        for d in range(1, reach + 1):

            @pl.when(hears(d))
            def _():
                tell(d).wait_recv()
                total[...] += lasts[d]

        weight = jnp.exp(total[0:1, :])
        for j in range(chunks):
            wts[j, 0:1, :] = jnp.where(
                left_row, weight[:, 2 * j : 2 * j + 1], weight[:, 2 * j + 1 : 2 * j + 2]
            )

    def step_a(j):
        @pl.when((pos != 0) & (pos != cut))
        def _():
            chain(j).wait_recv()

            @pl.when(pos < sp - 1)
            def _():
                a_out[j] = (a_in[j].astype(F32) * elast[j, 0:1, :] + local[j]).astype(BF16)

            @pl.when((pos != cut - 1) & (pos < sp - 1))
            def _():
                chain(j).start()

            @pl.when(pos == cut - 1)
            def _():
                cross(j).start()

    def step_b(j):
        @pl.when(pos < cut - 1)
        def _():
            back(j).wait_recv()
            b_out[j] = (b_in[j].astype(F32) + wts[j, 0:1, :] * local[j]).astype(BF16)
            back(j).start()

        @pl.when(pos >= cut)
        def _():
            carry_up(j).wait_recv()

            @pl.when(carries_up)
            def _():
                carry_up(j).start()

            @pl.when(carries_down)
            def _():
                carry_down(j).start()

    lag_a = jnp.where(first, HOP * pos, HOP * (pos - cut))
    lag_b = jnp.where(
        first,
        HOP * (cut - 1 - pos),
        jnp.where(pos < middle, HOP * pos, HOP * (cut + sp - 1 - pos)),
    )

    def flows(s):
        @pl.when((s >= lag_a) & (s < lag_a + groups))
        def _():
            for p in range(pairs):
                step_a((s - lag_a) * pairs + p)

        @pl.when((s >= lag_b) & (s < lag_b + groups))
        def _():
            for p in range(pairs):
                step_b((s - lag_b) * pairs + p)

    def inside(g):
        for p in range(pairs):
            local_columns = slice(p * LANES, (p + 1) * LANES)
            x_low = xlow[g, :, local_columns]
            h = g * ratio + 2 * p
            parts = []
            for i in range(2):
                gap = cum[:, h + i : h + i + 1] - cum_t[h + i : h + i + 1, :]
                weight = scores[g] * jnp.exp(jnp.where(causal, gap, -jnp.inf))
                parts.append(dot(weight.astype(BF16), x_low))
            inner[g, :, local_columns] = jnp.where(left_half, parts[0], parts[1])

    spread_lines()

    @pl.when(first)
    def _():
        weigh()

    for s in range(groups):
        flows(s)
        inside(s)

    @pl.when(jnp.logical_not(first))
    def _():
        weigh()

    sum_down = lax.broadcasted_iota(jnp.int32, (group_width, group_width), 0) // HEAD_DIM
    sum_across = lax.broadcasted_iota(jnp.int32, (group_width, group_width), 1) // HEAD_DIM
    averager = jnp.where(sum_down == sum_across, 1.0 / HEAD_DIM, 0.0).astype(BF16)

    def finish(g):
        entering = []
        for p in range(pairs):
            j = g * pairs + p
            more = jnp.where(first, 0.0, wts[j, 0:1, :] * b_in[j].astype(F32))
            entering.append((a_in[j].astype(F32) + more).astype(BF16))
        carried = dot(cact[g], jnp.concatenate(entering, axis=1))
        core_out = (inner[g] + ecum[g] * carried).astype(BF16)
        value = core_out.astype(F32) * zs[g]
        square = value * value
        high = square.astype(BF16)
        low = (square - high.astype(F32)).astype(BF16)
        mean = dot(high, averager) + dot(low, averager)
        gain = gain_ref[0:1, pl.ds(pl.multiple_of(g * group_width, group_width), group_width)]
        normed[g] = (value * lax.rsqrt(mean + NORM_EPS) * gain).astype(BF16)

    def project(g):
        start = pl.multiple_of(g * group_width, group_width)
        part = dot(normed[g], w_all[pl.ds(start, group_width), :])

        @pl.when(g == 0)
        def _():
            acc[...] = part

        @pl.when(g > 0)
        def _():
            acc[...] += part

    lag_f = jnp.maximum(jnp.maximum(lag_a, lag_b), groups)
    lag_p = jnp.maximum(lag_f, READY)

    def slot(s, carry):
        flows(s)
        for step, at in enumerate(RELAYS[:side]):

            @pl.when(s == at)
            def _():
                pass_rows(step)

        @pl.when(s == READY)
        def _():
            own.wait_recv()
            for axis in range(2):
                for k in range(side):
                    for i in range(side):
                        if k or i:
                            relay(axis, k, i).wait_recv()

        @pl.when((s >= lag_f) & (s < lag_f + groups))
        def _():
            finish(s - lag_f)

        @pl.when((s >= lag_p) & (s < lag_p + groups))
        def _():
            project(s - lag_p)

        return carry

    lax.fori_loop(groups, lag_p + groups, slot, 0)
    out_ref[0] = acc[...].astype(BF16)

    own.wait_send()
    for copy in shares:
        copy.wait_send()
    for axis in range(2):
        for i in steps:
            stage_one(axis, i).wait_send()
            for k in range(side):
                stage_two(axis, k, i).wait_send()
        for k in range(side):
            for i in range(side):
                if k or i:
                    relay(axis, k, i).wait_send()
    for d in range(1, reach + 1):

        @pl.when(tells(d))
        def _():
            tell(d).wait_send()

    @pl.when(pos < sp - 1)
    def _():
        for copy in halos:
            copy.wait_send()
        for j in range(chunks):
            chain(j).wait_send()

    @pl.when(first | carries_up | carries_down)
    def _():
        for j in range(chunks):
            back(j).wait_send()


def body(
    sp,
    dp,
    stream_x,
    stream_b,
    stream_c,
    gate_z,
    step_raw,
    conv_x,
    conv_b,
    conv_c,
    decay_log,
    norm_gain,
    w_out,
):
    tokens, width = stream_x.shape[1:]
    state_width = stream_b.shape[2]
    groups = state_width // STATE
    group_width = width // groups
    chunks = width // LANES
    columns = w_out.shape[1]
    side = math.isqrt(dp // 2)
    vmem = pl.BlockSpec(memory_space=pltpu.VMEM)
    anywhere = pl.BlockSpec(memory_space=pl.ANY)
    dma = pltpu.SemaphoreType.DMA
    return pl.pallas_call(
        functools.partial(kernel, sp, dp),
        out_shape=jax.ShapeDtypeStruct((1, tokens, columns), BF16),
        in_specs=[anywhere] * 4 + [vmem] + [anywhere] * 3 + [vmem] + [anywhere] * 2,
        out_specs=vmem,
        scratch_shapes=[
            pltpu.VMEM(conv_x.shape, BF16),
            pltpu.VMEM(conv_b.shape, BF16),
            pltpu.VMEM(conv_c.shape, BF16),
            pltpu.VMEM((1, width), F32),
            pltpu.VMEM((tokens, width), BF16),
            pltpu.VMEM((tokens, state_width), BF16),
            pltpu.VMEM((tokens, state_width), BF16),
            pltpu.VMEM((tokens, width), BF16),
            pltpu.VMEM((HALO, width), BF16),
            pltpu.VMEM((HALO, state_width), BF16),
            pltpu.VMEM((HALO, state_width), BF16),
            pltpu.VMEM((sp, 8, conv_x.shape[1] + LANES), F32),
            pltpu.VMEM((groups, 8, group_width + 2 * STATE), F32),
            pltpu.VMEM((LANES, tokens), F32),
            pltpu.VMEM((groups, tokens + 8, group_width + 2 * STATE), F32),
            pltpu.VMEM((groups, tokens, group_width), F32),
            pltpu.VMEM((groups, tokens, tokens), F32),
            pltpu.VMEM((groups, STATE, tokens), BF16),
            pltpu.VMEM((groups, tokens, group_width), BF16),
            pltpu.VMEM((groups, tokens, group_width), F32),
            pltpu.VMEM((groups, tokens, group_width), F32),
            pltpu.VMEM((chunks, 8, LANES), F32),
            pltpu.VMEM((chunks, 8, LANES), F32),
            pltpu.VMEM((sp, 8, LANES), F32),
            pltpu.VMEM((8, LANES), F32),
            pltpu.VMEM((groups, tokens, STATE), BF16),
            pltpu.VMEM((chunks, STATE, LANES), F32),
            pltpu.VMEM((chunks, STATE, LANES), BF16),
            pltpu.VMEM((chunks, STATE, LANES), BF16),
            pltpu.VMEM((chunks, STATE, LANES), BF16),
            pltpu.VMEM((chunks, STATE, LANES), BF16),
            pltpu.VMEM((groups, tokens, group_width), BF16),
            pltpu.VMEM((width, columns), BF16),
            pltpu.VMEM((tokens, columns), F32),
            dma((9,)),
            dma((sp,)),
            dma((sp,)),
            dma((sp,)),
            dma((sp,)),
            dma((3,)),
            dma((3,)),
            dma((chunks,)),
            dma((chunks,)),
            dma((chunks,)),
            dma((chunks,)),
            dma((2,)),
            dma((2, side)),
            dma((2, side)),
            dma((2, side, side)),
            dma((2, side, side)),
            dma((2, side, side)),
            dma((2, side, side)),
        ],
        compiler_params=pltpu.CompilerParams(
            collective_id=0, has_side_effects=True, vmem_limit_bytes=60 * 1024 * 1024
        ),
    )(
        stream_x,
        stream_b,
        stream_c,
        gate_z,
        jnp.swapaxes(step_raw, 1, 2),
        conv_x,
        conv_b,
        conv_c,
        decay_log.reshape(1, -1),
        norm_gain.reshape(1, -1),
        w_out,
    )


def solution(mesh):
    placed = (
        P("dp", "sp", None),
        P("dp", "sp", None),
        P("dp", "sp", None),
        P("dp", "sp", None),
        P("dp", "sp", None),
        P(None, "sp"),
        P(),
        P(),
        P("sp"),
        P(),
        P("dp", None),
    )
    return jax.shard_map(
        functools.partial(body, mesh.shape["sp"], mesh.shape["dp"]),
        mesh=mesh,
        in_specs=placed,
        out_specs=P("dp", "sp", None),
        check_vma=False,
    )
```

```python
import functools
import math

import jax
import jax.numpy as jnp
from jax import lax
from jax.experimental import pallas as pl
from jax.experimental.pallas import tpu as pltpu
from jax.sharding import PartitionSpec as P

HEAD_DIM = 64
STATE = 128
NORM_EPS = 1.0
HALO = 8
LANES = 128
HOP = 2
RELAYS = (8, 11, 14, 18)
F32 = jnp.float32
BF16 = jnp.bfloat16


def dot(a, b, precision=None):
    return jnp.dot(a, b, preferred_element_type=F32, precision=precision)


def silu(v):
    return v / (1.0 + jnp.exp(-v))


def kernel(
    sp,
    dp,
    x_hbm,
    b_hbm,
    c_hbm,
    z_hbm,
    raw_hbm,
    cx_hbm,
    cb_hbm,
    cc_hbm,
    dl_hbm,
    gain_hbm,
    w_hbm,
    out_ref,
    raw_ref,
    dl_ref,
    cx_ref,
    cb_ref,
    cc_ref,
    gain_ref,
    x_v,
    b_v,
    c_v,
    z_v,
    halo_x,
    halo_b,
    halo_c,
    par,
    tile,
    taps,
    wide_raw,
    ext,
    zs,
    scores,
    b_ts,
    xact,
    inner,
    ecum,
    elast,
    wts,
    lasts,
    total,
    cact,
    local,
    a_in,
    a_out,
    b_in,
    b_out,
    normed,
    w_all,
    in_sem,
    par_send,
    par_recv,
    last_send,
    last_recv,
    halo_send,
    halo_recv,
    a_send,
    a_recv,
    b_send,
    b_recv,
    own_sem,
    one_send,
    one_recv,
    two_send,
    two_recv,
    relay_send,
    relay_recv,
):
    tokens, inner_width = x_v.shape
    groups = b_v.shape[1] // STATE
    group_width = inner_width // groups
    pairs = group_width // LANES
    chunks = groups * pairs
    ratio = group_width // HEAD_DIM
    heads, local_heads = raw_ref.shape[0], dl_ref.shape[1]
    tap_count, tap_width = cx_ref.shape
    rows = w_hbm.shape[0]
    half_rows = rows // 2
    side = math.isqrt(dp // 2)
    cut = max(2, (3 * sp) // 8)
    middle = cut + (sp - cut + 1) // 2
    reach = max(cut, sp - cut) - 1

    pos = lax.axis_index("sp")
    me = lax.axis_index("dp")
    core = me % 2
    partner = me + 1 - 2 * core
    place = me // 2
    column, line = place % side, place // side
    following = (pos + 1) % sp
    preceding = (pos + sp - 1) % sp
    first = pos < cut

    def remote(src, dst, send, recv, target):
        return pltpu.make_async_remote_copy(
            src_ref=src,
            dst_ref=dst,
            send_sem=send,
            recv_sem=recv,
            device_id=target,
            device_id_type=pl.DeviceIdType.MESH,
        )

    def chip(axis, along, across):
        dx, dy = (along, across) if axis == 0 else (across, along)
        return ((line + dy + side) % side) * side + (column + dx + side) % side

    barrier = pltpu.get_barrier_semaphore()
    greeted = [{"sp": (pos + j) % sp} for j in range(1, sp)] + [{"dp": partner}]
    for axis in range(2):
        for i in range(1, side):
            greeted.append({"dp": 2 * chip(axis, i, 0) + core})
    for target in greeted:
        pl.semaphore_signal(
            barrier, inc=1, device_id=target, device_id_type=pl.DeviceIdType.MESH
        )

    sources = (
        (cx_hbm, cx_ref),
        (dl_hbm, dl_ref),
        (raw_hbm.at[0], raw_ref),
        (b_hbm.at[0], b_v),
        (c_hbm.at[0], c_v),
        (x_hbm.at[0], x_v),
        (cb_hbm, cb_ref),
        (cc_hbm, cc_ref),
        (z_hbm.at[0], z_v),
        (gain_hbm, gain_ref),
    )
    loads = [
        pltpu.make_async_copy(src, dst, in_sem.at[i]) for i, (src, dst) in enumerate(sources)
    ]
    for load in loads:
        load.start()

    def piece(axis, along, across):
        origin = 2 * chip(axis, along, across) + core
        start = pl.multiple_of(origin * rows + axis * half_rows, half_rows)
        return w_all.at[pl.ds(start, half_rows), :]

    own_rows = w_all.at[pl.ds(pl.multiple_of(me * rows, rows), rows), :]
    keep = pltpu.make_async_copy(w_hbm, own_rows, in_sem.at[len(sources)])
    keep.start()

    wide_raw[...] = jnp.zeros(wide_raw.shape, F32)
    for load in loads[0:3]:
        load.wait()
    wide_raw[0:1, 0:local_heads] = dl_ref[...]
    decays = pltpu.roll(wide_raw[0:8, :], pos * local_heads, 1)[0:1, :]
    tile[...] = jnp.zeros(tile.shape, F32)
    tile[0:tap_count, :] = cx_ref[...].astype(F32)
    for i in range(3):
        part = decays.astype(BF16).astype(F32)
        tile[tap_count + i : tap_count + i + 1, :] = part
        decays = decays - part
    par[pos] = tile[...].astype(BF16)
    wide_raw[0:heads, :] = raw_ref[...].astype(F32)
    for load in loads[3:]:
        load.wait()
    keep.wait()
    pl.semaphore_wait(barrier, len(greeted))

    halos = [
        remote(
            src.at[pl.ds(tokens - HALO, HALO), :],
            dst,
            halo_send.at[i],
            halo_recv.at[i],
            {"sp": following},
        )
        for i, (src, dst) in enumerate(((x_v, halo_x), (b_v, halo_b), (c_v, halo_c)))
    ]

    @pl.when(pos < sp - 1)
    def _():
        for copy in halos:
            copy.start()

    shares = [
        remote(
            par.at[pos],
            par.at[pos],
            par_send.at[j - 1],
            par_recv.at[j - 1],
            {"sp": (pos + j) % sp},
        )
        for j in range(1, sp)
    ]
    for copy in shares:
        copy.start()

    def stage_one(axis, i):
        return remote(
            piece(axis, 0, 0),
            piece(axis, 0, 0),
            one_send.at[axis, i],
            one_recv.at[axis, i],
            {"dp": 2 * chip(axis, i, 0) + core},
        )

    def stage_two(axis, k, i):
        return remote(
            piece(axis, -k, 0),
            piece(axis, -k, 0),
            two_send.at[axis, k, i],
            two_recv.at[axis, k, i],
            {"dp": 2 * chip(axis, 0, i) + core},
        )

    def relay(axis, k, i):
        return remote(
            piece(axis, -k, -i),
            piece(axis, -k, -i),
            relay_send.at[axis, k, i],
            relay_recv.at[axis, k, i],
            {"dp": partner},
        )

    steps = sorted(range(1, side), key=lambda i: min(i, side - i))
    for i in steps:
        for axis in range(2):
            stage_one(axis, i).start()
    for i in steps:
        for axis in range(2):
            stage_two(axis, 0, i).start()
    own = remote(own_rows, own_rows, own_sem.at[0], own_sem.at[1], {"dp": partner})
    own.start()

    def spread_lines():
        for k in steps:
            for axis in range(2):
                stage_one(axis, k).wait_recv()
                for i in steps:
                    stage_two(axis, k, i).start()

    def pass_rows(step):
        if step == 0:
            for k in steps:
                for axis in range(2):
                    relay(axis, k, 0).start()
            which = 0
        else:
            which = steps[step - 1]
        for i in steps:
            for axis in range(2):
                stage_two(axis, which, i).wait_recv()
                relay(axis, which, i).start()

    raw = jnp.transpose(wide_raw[...])
    dt = jnp.maximum(raw, 0.0) + jnp.log(1.0 + jnp.exp(-jnp.abs(raw)))
    down = lax.broadcasted_iota(jnp.int32, (tokens, tokens), 0)
    across_tokens = lax.broadcasted_iota(jnp.int32, (tokens, tokens), 1)
    causal = down >= across_tokens
    left_half = lax.broadcasted_iota(jnp.int32, (tokens, LANES), 1) < HEAD_DIM
    left_row = left_half[0:1, :]
    for g in range(groups):
        taps[g, 0:tap_count, group_width : group_width + STATE] = cb_ref[
            :, g * STATE : (g + 1) * STATE
        ].astype(F32)
        taps[g, 0:tap_count, group_width + STATE : group_width + 2 * STATE] = cc_ref[
            :, g * STATE : (g + 1) * STATE
        ].astype(F32)
        zs[g] = silu(z_v[:, g * group_width : (g + 1) * group_width].astype(F32))

    @pl.when(pos == 0)
    def _():
        ext[:, 0:8, :] = jnp.zeros((groups, 8, ext.shape[2]), F32)

    @pl.when((pos == 0) | (pos == cut))
    def _():
        a_in[...] = jnp.zeros(a_in.shape, BF16)

    @pl.when(pos > 0)
    def _():
        for copy in halos:
            copy.wait_recv()
        for g in range(groups):
            wide = slice(g * group_width, (g + 1) * group_width)
            thin = slice(g * STATE, (g + 1) * STATE)
            ext[g, 0:8, 0:group_width] = halo_x[:, wide].astype(F32)
            ext[g, 0:8, group_width : group_width + STATE] = halo_b[:, thin].astype(F32)
            ext[g, 0:8, group_width + STATE :] = halo_c[:, thin].astype(F32)

    def conv(g, source, at):
        columns = slice(at, at + LANES)
        ext[g, 8 : 8 + tokens, columns] = source.astype(F32)
        summed = taps[g, 0:1, columns] * ext[g, 9 - tap_count : 9 - tap_count + tokens, columns]
        for k in range(1, tap_count):
            start = 9 - tap_count + k
            summed = summed + taps[g, k : k + 1, columns] * ext[g, start : start + tokens, columns]
        return silu(summed).astype(BF16)

    for g in range(groups):
        thin = slice(g * STATE, (g + 1) * STATE)
        b_act = conv(g, b_v[:, thin], group_width)
        c_act = conv(g, c_v[:, thin], group_width + STATE)
        cact[g] = c_act
        b_t = jnp.transpose(b_act)
        b_ts[g] = b_t
        scores[g] = dot(c_act, b_t)

    for copy in shares:
        copy.wait_recv()
    gathered = par[0].astype(F32)
    for s in range(1, sp):
        gathered = gathered + par[s].astype(F32)
    rates = gathered[tap_count : tap_count + 1, :]
    for i in range(1, 3):
        rates = rates + gathered[tap_count + i : tap_count + i + 1, :]
    log_decay = dt * (-jnp.exp(rates))
    cum = dot(jnp.where(causal, 1.0, 0.0).astype(F32), log_decay, lax.Precision.HIGHEST)
    cum_t = jnp.transpose(cum)
    last = cum[tokens - 1 : tokens, :]
    lasts[0] = jnp.broadcast_to(last, lasts.shape[1:])
    tail = dt * jnp.exp(last - cum)

    def tell(d):
        target = jnp.where(first, pos + sp - d, pos + d) % sp
        return remote(
            lasts.at[0], lasts.at[d], last_send.at[d], last_recv.at[d], {"sp": target}
        )

    def tells(d):
        return (first & (pos >= d)) | (jnp.logical_not(first) & (pos + d < sp))

    def hears(d):
        return (first & (pos + d < cut)) | (jnp.logical_not(first) & (pos - d >= cut))

    for d in range(1, reach + 1):

        @pl.when(tells(d))
        def _():
            tell(d).start()

    for chunk in range(chunks):
        begin = chunk * LANES
        g, at = begin // group_width, begin % group_width
        s = begin // tap_width
        taps[g, 0:tap_count, at : at + LANES] = par[s].astype(F32)[0:tap_count, :]

    def chain(j):
        return remote(a_out.at[j], a_in.at[j], a_send.at[j], a_recv.at[j], {"sp": following})

    def cross(j):
        return remote(a_out.at[j], b_in.at[j], a_send.at[j], b_recv.at[j], {"sp": following})

    def back(j):
        return remote(b_out.at[j], b_in.at[j], b_send.at[j], b_recv.at[j], {"sp": preceding})

    def carry_up(j):
        return remote(b_in.at[j], b_in.at[j], b_send.at[j], b_recv.at[j], {"sp": following})

    def carry_down(j):
        return remote(b_in.at[j], b_in.at[j], b_send.at[j], b_recv.at[j], {"sp": preceding})

    carries_up = (pos >= cut) & (pos < middle - 1)
    carries_down = pos > middle

    def spread_rows(rows_ref, values):
        for j in range(chunks):
            rows_ref[j, 0:1, :] = jnp.where(
                left_row, values[:, 2 * j : 2 * j + 1], values[:, 2 * j + 1 : 2 * j + 2]
            )

    def spread_columns(values, h):
        return jnp.where(left_half, values[:, h : h + 1], values[:, h + 1 : h + 2])

    def states(g):
        b_t = b_ts[g]
        for p in range(pairs):
            j = g * pairs + p
            x_act = conv(g, x_v[:, j * LANES : (j + 1) * LANES], p * LANES)
            xact[g, :, p * LANES : (p + 1) * LANES] = x_act
            x_tail = (x_act.astype(F32) * spread_columns(tail, 2 * j)).astype(BF16)
            local[j] = dot(b_t, x_tail)

    def begin_flows(some, which):
        @pl.when((core == which) & ((pos == 0) | (pos == cut)))
        def _():
            for g in some:
                for j in range(g * pairs, (g + 1) * pairs):
                    a_out[j] = local[j].astype(BF16)
                    chain(j).start()

        @pl.when((core == which) & (pos == cut - 1))
        def _():
            for g in some:
                for j in range(g * pairs, (g + 1) * pairs):
                    b_out[j] = local[j].astype(BF16)
                    back(j).start()

    for number, some in enumerate(([0], range(1, groups // 2), range(groups // 2, groups))):
        for g in some:
            states(g)
        if number == 0:
            spread_rows(elast, jnp.exp(last))
        begin_flows(some, 0)

    def weigh():
        total[...] = jnp.zeros(total.shape, F32)
        for d in range(1, reach + 1):

            @pl.when(hears(d))
            def _():
                tell(d).wait_recv()
                total[...] += lasts[d]

        spread_rows(wts, jnp.exp(total[0:1, :]))

    def step_a(j):
        @pl.when((pos != 0) & (pos != cut))
        def _():
            chain(j).wait_recv()

            @pl.when(pos < sp - 1)
            def _():
                a_out[j] = (a_in[j].astype(F32) * elast[j, 0:1, :] + local[j]).astype(BF16)

            @pl.when((pos != cut - 1) & (pos < sp - 1))
            def _():
                chain(j).start()

            @pl.when(pos == cut - 1)
            def _():
                cross(j).start()

    def step_b(j):
        @pl.when(pos < cut - 1)
        def _():
            back(j).wait_recv()
            b_out[j] = (b_in[j].astype(F32) + wts[j, 0:1, :] * local[j]).astype(BF16)
            back(j).start()

        @pl.when(pos >= cut)
        def _():
            carry_up(j).wait_recv()

            @pl.when(carries_up)
            def _():
                carry_up(j).start()

            @pl.when(carries_down)
            def _():
                carry_down(j).start()

    lag_a = jnp.where(first, HOP * pos, HOP * (pos - cut))
    lag_b = jnp.where(
        first,
        HOP * (cut - 1 - pos),
        jnp.where(pos < middle, HOP * pos, HOP * (cut + sp - 1 - pos)),
    )

    def flows(s):
        @pl.when((s >= lag_a) & (s < lag_a + groups))
        def _():
            for p in range(pairs):
                step_a((s - lag_a) * pairs + p)

        @pl.when((s >= lag_b) & (s < lag_b + groups))
        def _():
            for p in range(pairs):
                step_b((s - lag_b) * pairs + p)

    def inside(g):
        for p in range(pairs):
            local_columns = slice(p * LANES, (p + 1) * LANES)
            h = g * ratio + 2 * p
            x_dt = xact[g, :, local_columns].astype(F32) * spread_columns(dt, h)
            x_low = x_dt.astype(BF16)
            parts = []
            spread = []
            for i in range(2):
                spread.append(jnp.broadcast_to(cum[:, h + i : h + i + 1], (tokens, LANES)))
                gap = spread[i] - cum_t[h + i : h + i + 1, :]
                weight = scores[g] * jnp.exp(jnp.where(causal, gap, -jnp.inf))
                parts.append(dot(weight.astype(BF16), x_low))
            inner[g, :, local_columns] = jnp.where(left_half, parts[0], parts[1])
            ecum[g, :, local_columns] = jnp.exp(jnp.where(left_half, spread[0], spread[1]))

    for s in range(groups):
        if s == 0 or s == groups // 2:

            @pl.when(first & ((pos >= cut - 2) if s == 0 else (pos < cut - 2)))
            def _():
                weigh()

        flows(s)
        inside(s)
        if s == 0:
            spread_lines()
    begin_flows(range(groups), 1)

    sum_down = lax.broadcasted_iota(jnp.int32, (group_width, group_width), 0) // HEAD_DIM
    sum_across = lax.broadcasted_iota(jnp.int32, (group_width, group_width), 1) // HEAD_DIM
    averager = jnp.where(sum_down == sum_across, 1.0 / HEAD_DIM, 0.0).astype(BF16)

    def finish(g):
        entering = []
        for p in range(pairs):
            j = g * pairs + p
            more = jnp.where(first, 0.0, wts[j, 0:1, :] * b_in[j].astype(F32))
            entering.append((a_in[j].astype(F32) + more).astype(BF16))
        carried = dot(cact[g], jnp.concatenate(entering, axis=1))
        core_out = (inner[g] + ecum[g] * carried).astype(BF16)
        value = core_out.astype(F32) * zs[g]
        square = value * value
        high = square.astype(BF16)
        low = (square - high.astype(F32)).astype(BF16)
        mean = dot(high, averager) + dot(low, averager)
        gain = gain_ref[0:1, pl.ds(pl.multiple_of(g * group_width, group_width), group_width)]
        normed[g] = (value * lax.rsqrt(mean + NORM_EPS) * gain).astype(BF16)

    lag_f = jnp.maximum(jnp.maximum(lag_a, lag_b), groups)
    slots = jnp.maximum(lag_f + groups, RELAYS[side - 1] + 1)

    def slot(s, carry):
        flows(s)
        for step, at in enumerate(RELAYS[:side]):

            @pl.when(s == at)
            def _():
                pass_rows(step)

        @pl.when(jnp.logical_not(first) & (s == lag_f))
        def _():
            weigh()

        @pl.when((s >= lag_f) & (s < lag_f + groups))
        def _():
            finish(s - lag_f)

        return carry

    lax.fori_loop(groups, slots, slot, 0)

    own.wait_recv()
    for axis in range(2):
        for k in range(side):
            for i in range(side):
                if k or i:
                    relay(axis, k, i).wait_recv()
    result = dot(normed[0], w_all[0:group_width, :])
    for g in range(1, groups):
        result += dot(normed[g], w_all[g * group_width : (g + 1) * group_width, :])
    out_ref[0] = result.astype(BF16)

    own.wait_send()
    for copy in shares:
        copy.wait_send()
    for axis in range(2):
        for i in steps:
            stage_one(axis, i).wait_send()
            for k in range(side):
                stage_two(axis, k, i).wait_send()
        for k in range(side):
            for i in range(side):
                if k or i:
                    relay(axis, k, i).wait_send()
    for d in range(1, reach + 1):

        @pl.when(tells(d))
        def _():
            tell(d).wait_send()

    @pl.when(pos < sp - 1)
    def _():
        for copy in halos:
            copy.wait_send()
        for j in range(chunks):
            chain(j).wait_send()

    @pl.when(first | carries_up | carries_down)
    def _():
        for j in range(chunks):
            back(j).wait_send()


def body(
    sp,
    dp,
    stream_x,
    stream_b,
    stream_c,
    gate_z,
    step_raw,
    conv_x,
    conv_b,
    conv_c,
    decay_log,
    norm_gain,
    w_out,
):
    tokens, width = stream_x.shape[1:]
    state_width = stream_b.shape[2]
    groups = state_width // STATE
    group_width = width // groups
    chunks = width // LANES
    columns = w_out.shape[1]
    side = math.isqrt(dp // 2)
    vmem = pl.BlockSpec(memory_space=pltpu.VMEM)
    anywhere = pl.BlockSpec(memory_space=pl.ANY)
    dma = pltpu.SemaphoreType.DMA
    return pl.pallas_call(
        functools.partial(kernel, sp, dp),
        out_shape=jax.ShapeDtypeStruct((1, tokens, columns), BF16),
        in_specs=[anywhere] * 11,
        out_specs=vmem,
        scratch_shapes=[
            pltpu.VMEM((step_raw.shape[2], tokens), BF16),
            pltpu.VMEM((1, decay_log.shape[0]), F32),
            pltpu.VMEM(conv_x.shape, BF16),
            pltpu.VMEM(conv_b.shape, BF16),
            pltpu.VMEM(conv_c.shape, BF16),
            pltpu.VMEM((1, width), F32),
            pltpu.VMEM((tokens, width), BF16),
            pltpu.VMEM((tokens, state_width), BF16),
            pltpu.VMEM((tokens, state_width), BF16),
            pltpu.VMEM((tokens, width), BF16),
            pltpu.VMEM((HALO, width), BF16),
            pltpu.VMEM((HALO, state_width), BF16),
            pltpu.VMEM((HALO, state_width), BF16),
            pltpu.VMEM((sp, 8, LANES), BF16),
            pltpu.VMEM((8, LANES), F32),
            pltpu.VMEM((groups, 8, group_width + 2 * STATE), F32),
            pltpu.VMEM((LANES, tokens), F32),
            pltpu.VMEM((groups, tokens + 8, group_width + 2 * STATE), F32),
            pltpu.VMEM((groups, tokens, group_width), F32),
            pltpu.VMEM((groups, tokens, tokens), F32),
            pltpu.VMEM((groups, STATE, tokens), BF16),
            pltpu.VMEM((groups, tokens, group_width), BF16),
            pltpu.VMEM((groups, tokens, group_width), F32),
            pltpu.VMEM((groups, tokens, group_width), F32),
            pltpu.VMEM((chunks, 8, LANES), F32),
            pltpu.VMEM((chunks, 8, LANES), F32),
            pltpu.VMEM((sp, 8, LANES), F32),
            pltpu.VMEM((8, LANES), F32),
            pltpu.VMEM((groups, tokens, STATE), BF16),
            pltpu.VMEM((chunks, STATE, LANES), F32),
            pltpu.VMEM((chunks, STATE, LANES), BF16),
            pltpu.VMEM((chunks, STATE, LANES), BF16),
            pltpu.VMEM((chunks, STATE, LANES), BF16),
            pltpu.VMEM((chunks, STATE, LANES), BF16),
            pltpu.VMEM((groups, tokens, group_width), BF16),
            pltpu.VMEM((width, columns), BF16),
            dma((11,)),
            dma((sp,)),
            dma((sp,)),
            dma((sp,)),
            dma((sp,)),
            dma((3,)),
            dma((3,)),
            dma((chunks,)),
            dma((chunks,)),
            dma((chunks,)),
            dma((chunks,)),
            dma((2,)),
            dma((2, side)),
            dma((2, side)),
            dma((2, side, side)),
            dma((2, side, side)),
            dma((2, side, side)),
            dma((2, side, side)),
        ],
        compiler_params=pltpu.CompilerParams(
            collective_id=0, has_side_effects=True, vmem_limit_bytes=60 * 1024 * 1024
        ),
    )(
        stream_x,
        stream_b,
        stream_c,
        gate_z,
        jnp.swapaxes(step_raw, 1, 2),
        conv_x,
        conv_b,
        conv_c,
        decay_log.reshape(1, -1),
        norm_gain.reshape(1, -1),
        w_out,
    )


def solution(mesh):
    placed = (
        P("dp", "sp", None),
        P("dp", "sp", None),
        P("dp", "sp", None),
        P("dp", "sp", None),
        P("dp", "sp", None),
        P(None, "sp"),
        P(),
        P(),
        P("sp"),
        P(),
        P("dp", None),
    )
    return jax.shard_map(
        functools.partial(body, mesh.shape["sp"], mesh.shape["dp"]),
        mesh=mesh,
        in_specs=placed,
        out_specs=P("dp", "sp", None),
        check_vma=False,
    )
```

```python
import functools
import math

import jax
import jax.numpy as jnp
from jax import lax
from jax.experimental import pallas as pl
from jax.experimental.pallas import tpu as pltpu
from jax.sharding import PartitionSpec as P

HEAD_DIM = 64
STATE = 128
NORM_EPS = 1.0
HALO = 8
LANES = 128
HOP = 4
UP_SLOTS = (5, 7, 11, 16, 21, 23, 24, 26)
BACK_SLOTS = (13, 16, 18, 20, 23, 25, 26, 28)
UP_STATES = (2, 6, 11, 15, 19)
BACK_STATES = (12, 14, 15, 16, 20)
STATES_END = 23
FINISH = 31
RELAYS = (31, 34, 39, 45)
LATER = 7
LATE_SLOTS = (19, 20, 21, 22, 23, 25, 26, 28)
BEHIND = 4
CUBE = 4
F32 = jnp.float32
BF16 = jnp.bfloat16


def dot(a, b, precision=None):
    return jnp.dot(a, b, preferred_element_type=F32, precision=precision)


def silu(v):
    return v / (1.0 + jnp.exp(-v))


def kernel(
    sp,
    dp,
    x_hbm,
    b_hbm,
    c_hbm,
    z_hbm,
    raw_hbm,
    cx_hbm,
    cb_hbm,
    cc_hbm,
    dl_hbm,
    gain_hbm,
    w_hbm,
    out_hbm,
    raw_ref,
    dl_ref,
    cx_ref,
    cb_ref,
    cc_ref,
    gain_ref,
    x_v,
    b_v,
    c_v,
    z_v,
    halo_x,
    halo_b,
    halo_c,
    par,
    tile,
    taps,
    wide_raw,
    ext,
    zs,
    scores,
    b_ts,
    xact,
    inner,
    ecum,
    elast,
    wts,
    lasts,
    total,
    rates,
    cact,
    local,
    a_in,
    a_out,
    b_in,
    b_out,
    normed,
    w_all,
    in_sem,
    par_send,
    par_recv,
    last_send,
    last_recv,
    halo_send,
    halo_recv,
    a_send,
    a_recv,
    b_send,
    b_recv,
    own_sem,
    one_send,
    one_recv,
    two_send,
    two_recv,
    relay_send,
    relay_recv,
    out_v,
    out_send,
):
    tokens, inner_width = x_v.shape
    groups = b_v.shape[1] // STATE
    group_width = inner_width // groups
    pairs = group_width // LANES
    chunks = groups * pairs
    ratio = group_width // HEAD_DIM
    heads, local_heads = raw_ref.shape[0], dl_ref.shape[1]
    tap_count, tap_width = cx_ref.shape
    rows = w_hbm.shape[0]
    half_rows = rows // 2
    side = math.isqrt(dp // 2)
    cut = max(2, (3 * sp) // 8)
    middle = cut + (sp - cut + 1) // 2 + (1 if sp > 8 else 0)
    reach = max(cut, sp - cut) - 1

    pos = lax.axis_index("sp")
    me = lax.axis_index("dp")
    core = me % 2
    partner = me + 1 - 2 * core
    place = me // 2
    column, line = place % side, place // side
    following = (pos + 1) % sp
    preceding = (pos + sp - 1) % sp
    first = pos < cut

    def remote(src, dst, send, recv, target):
        return pltpu.make_async_remote_copy(
            src_ref=src,
            dst_ref=dst,
            send_sem=send,
            recv_sem=recv,
            device_id=target,
            device_id_type=pl.DeviceIdType.MESH,
        )

    def chip(axis, along, across):
        dx, dy = (along, across) if axis == 0 else (across, along)
        return ((line + dy + side) % side) * side + (column + dx + side) % side

    barrier = pltpu.get_barrier_semaphore()
    for j in range(1, sp):

        @pl.when(pos + j < sp)
        def _():
            pl.semaphore_signal(
                barrier,
                inc=1,
                device_id={"sp": (pos + j) % sp},
                device_id_type=pl.DeviceIdType.MESH,
            )

    @pl.when(pos > 0)
    def _():
        pl.semaphore_signal(
            barrier, inc=1, device_id={"sp": preceding}, device_id_type=pl.DeviceIdType.MESH
        )

    greeted = [{"dp": partner}]
    for axis in range(2):
        for i in range(1, side):
            greeted.append({"dp": 2 * chip(axis, i, 0) + core})
    for target in greeted:
        pl.semaphore_signal(
            barrier, inc=1, device_id=target, device_id_type=pl.DeviceIdType.MESH
        )

    sources = (
        (cx_hbm, cx_ref),
        (dl_hbm, dl_ref),
        (raw_hbm.at[0], raw_ref),
        (b_hbm.at[0], b_v),
        (c_hbm.at[0], c_v),
        (x_hbm.at[0], x_v),
        (cb_hbm, cb_ref),
        (cc_hbm, cc_ref),
        (z_hbm.at[0], z_v),
        (gain_hbm, gain_ref),
    )
    loads = [
        pltpu.make_async_copy(src, dst, in_sem.at[i]) for i, (src, dst) in enumerate(sources)
    ]
    for load in loads:
        load.start()

    def piece(axis, along, across):
        origin = 2 * chip(axis, along, across) + core
        start = pl.multiple_of(origin * rows + axis * half_rows, half_rows)
        return w_all.at[pl.ds(start, half_rows), :]

    own_rows = w_all.at[pl.ds(pl.multiple_of(me * rows, rows), rows), :]
    keep = pltpu.make_async_copy(w_hbm, own_rows, in_sem.at[len(sources)])
    keep.start()

    wide_raw[...] = jnp.zeros(wide_raw.shape, F32)
    for load in loads[0:3]:
        load.wait()
    wide_raw[0:1, 0:local_heads] = dl_ref[...]
    decays = pltpu.roll(wide_raw[0:8, :], pos * local_heads, 1)[0:1, :]
    tile[...] = jnp.zeros(tile.shape, F32)
    tile[0:tap_count, :] = cx_ref[...].astype(F32)
    for i in range(3):
        part = decays.astype(BF16).astype(F32)
        tile[tap_count + i : tap_count + i + 1, :] = part
        decays = decays - part
    par[pos] = tile[...].astype(BF16)
    wide_raw[0:heads, :] = raw_ref[...].astype(F32)
    for load in loads[3:]:
        load.wait()
    keep.wait()
    pl.semaphore_wait(barrier, len(greeted) + jnp.minimum(pos + 1, sp - 1))

    halos = [
        remote(
            src.at[pl.ds(tokens - HALO, HALO), :],
            dst,
            halo_send.at[i],
            halo_recv.at[i],
            {"sp": following},
        )
        for i, (src, dst) in enumerate(((x_v, halo_x), (b_v, halo_b), (c_v, halo_c)))
    ]

    @pl.when(pos < sp - 1)
    def _():
        for copy in halos:
            copy.start()

    def share(target):
        return remote(
            par.at[pos], par.at[pos], par_send.at[target], par_recv.at[pos], {"sp": target}
        )

    for j in range(1, sp):

        @pl.when(pos >= j)
        def _():
            share((pos + sp - j) % sp).start()

    @pl.when(pos < sp - 1)
    def _():
        share(following).start()

    def early(source):
        return (pos > 0) & (pos + 1 < source) & (source < cut)

    def hear(source, now):
        if not isinstance(now, bool):
            now = now & (pos != source)
        else:
            now = (pos != source) & jnp.logical_not(early(source))

        @pl.when(now)
        def _():
            remote(
                par.at[source],
                par.at[source],
                par_send.at[source],
                par_recv.at[source],
                {"sp": source},
            ).wait_recv()

        @pl.when(now & (pos + 1 < source))
        def _():
            share(source).start()

    def stage_one(axis, i):
        return remote(
            piece(axis, 0, 0),
            piece(axis, 0, 0),
            one_send.at[axis, i],
            one_recv.at[axis, i],
            {"dp": 2 * chip(axis, i, 0) + core},
        )

    def stage_two(axis, k, i):
        return remote(
            piece(axis, -k, 0),
            piece(axis, -k, 0),
            two_send.at[axis, k, i],
            two_recv.at[axis, k, i],
            {"dp": 2 * chip(axis, 0, i) + core},
        )

    def relay(axis, k, i):
        return remote(
            piece(axis, -k, -i),
            piece(axis, -k, -i),
            relay_send.at[axis, k, i],
            relay_recv.at[axis, k, i],
            {"dp": partner},
        )

    steps = sorted(range(1, side), key=lambda i: min(i, side - i))
    for i in steps:
        for axis in range(2):
            stage_one(axis, i).start()
    for i in steps:
        for axis in range(2):
            stage_two(axis, 0, i).start()
    own = remote(own_rows, own_rows, own_sem.at[0], own_sem.at[1], {"dp": partner})
    own.start()

    def spread_lines():
        for k in steps:
            for axis in range(2):
                stage_one(axis, k).wait_recv()
                for i in steps:
                    stage_two(axis, k, i).start()

    def pass_rows(step):
        if step == 0:
            for k in steps:
                for axis in range(2):
                    relay(axis, k, 0).start()
            which = 0
        else:
            which = steps[step - 1]
        for i in steps:
            for axis in range(2):
                stage_two(axis, which, i).wait_recv()
                relay(axis, which, i).start()

    raw = jnp.transpose(wide_raw[...])
    dt = jnp.maximum(raw, 0.0) + jnp.log(1.0 + jnp.exp(-jnp.abs(raw)))
    down = lax.broadcasted_iota(jnp.int32, (tokens, tokens), 0)
    across_tokens = lax.broadcasted_iota(jnp.int32, (tokens, tokens), 1)
    causal = down >= across_tokens
    left_half = lax.broadcasted_iota(jnp.int32, (tokens, LANES), 1) < HEAD_DIM
    left_row = left_half[0:1, :]
    for g in range(groups):
        taps[g, 0:tap_count, group_width : group_width + STATE] = cb_ref[
            :, g * STATE : (g + 1) * STATE
        ].astype(F32)
        taps[g, 0:tap_count, group_width + STATE : group_width + 2 * STATE] = cc_ref[
            :, g * STATE : (g + 1) * STATE
        ].astype(F32)
        zs[g] = silu(z_v[:, g * group_width : (g + 1) * group_width].astype(F32))

    @pl.when(pos == 0)
    def _():
        ext[:, 0:8, :] = jnp.zeros((groups, 8, ext.shape[2]), F32)

    causal_ones = jnp.where(causal, 1.0, 0.0).astype(F32)
    steps_sum = dot(causal_ones, dt, lax.Precision.HIGHEST)
    rates[...] = jnp.zeros(rates.shape, F32)

    @pl.when((pos == 0) | (pos == cut))
    def _():
        a_in[...] = jnp.zeros(a_in.shape, BF16)

    @pl.when(pos > 0)
    def _():
        for copy in halos:
            copy.wait_recv()
        for g in range(groups):
            wide = slice(g * group_width, (g + 1) * group_width)
            thin = slice(g * STATE, (g + 1) * STATE)
            ext[g, 0:8, 0:group_width] = halo_x[:, wide].astype(F32)
            ext[g, 0:8, group_width : group_width + STATE] = halo_b[:, thin].astype(F32)
            ext[g, 0:8, group_width + STATE :] = halo_c[:, thin].astype(F32)

    def conv(g, source, at):
        columns = slice(at, at + LANES)
        ext[g, 8 : 8 + tokens, columns] = source.astype(F32)
        summed = taps[g, 0:1, columns] * ext[g, 9 - tap_count : 9 - tap_count + tokens, columns]
        for k in range(1, tap_count):
            start = 9 - tap_count + k
            summed = summed + taps[g, k : k + 1, columns] * ext[g, start : start + tokens, columns]
        return silu(summed).astype(BF16)

    for g in range(groups):
        thin = slice(g * STATE, (g + 1) * STATE)
        b_act = conv(g, b_v[:, thin], group_width)
        c_act = conv(g, c_v[:, thin], group_width + STATE)
        cact[g] = c_act
        b_t = jnp.transpose(b_act)
        b_ts[g] = b_t
        scores[g] = dot(c_act, b_t)

    def ranked(center):
        near = lambda g: abs((g + 0.5) * per - center)
        return sorted(range(groups), key=near)

    def staged(order):
        single = min(4, groups - 1)
        return [[g] for g in order[:single]] + [order[single:]]

    per = group_width // tap_width
    back_order = ranked(cut + 1.2)
    up_stages, back_stages = staged(list(range(groups))), staged(back_order)
    stages = len(up_stages)

    def back_group(k):
        g = jnp.int32(back_order[0])
        for i in range(1, groups):
            g = jnp.where(k == i, back_order[i], g)
        return g

    def tell(d, i):
        target = jnp.where(first, pos + sp - d, pos + d) % sp
        return remote(
            lasts.at[0, i], lasts.at[d, i], last_send.at[d, i], last_recv.at[d, i], {"sp": target}
        )

    def tells(d, i):
        later = jnp.logical_not(first) & (pos + d < sp)
        return (first & (pos >= d)) | (later if i == stages - 1 else False)

    def chain(j):
        return remote(a_out.at[j], a_in.at[j], a_send.at[j], a_recv.at[j], {"sp": following})

    def cross(j):
        return remote(a_out.at[j], b_in.at[j], a_send.at[j], b_recv.at[j], {"sp": following})

    def back(j):
        return remote(b_out.at[j], b_in.at[j], b_send.at[j], b_recv.at[j], {"sp": preceding})

    def carry_up(j):
        return remote(b_in.at[j], b_in.at[j], b_send.at[j], b_recv.at[j], {"sp": following})

    def carry_down(j):
        return remote(b_in.at[j], b_in.at[j], b_send.at[j], b_recv.at[j], {"sp": preceding})

    carries_up = (pos >= cut) & (pos < middle - 1)
    carries_down = pos > middle

    def spread_rows(rows_ref, values):
        for j in range(chunks):
            rows_ref[j, 0:1, :] = jnp.where(
                left_row, values[:, 2 * j : 2 * j + 1], values[:, 2 * j + 1 : 2 * j + 2]
            )

    def spread_columns(values, h):
        return jnp.where(left_half, values[:, h : h + 1], values[:, h + 1 : h + 2])

    def states(g, tail):
        b_t = b_ts[g]
        for p in range(pairs):
            j = g * pairs + p
            x_act = conv(g, x_v[:, j * LANES : (j + 1) * LANES], p * LANES)
            xact[g, :, p * LANES : (p + 1) * LANES] = x_act
            x_tail = (x_act.astype(F32) * spread_columns(tail, 2 * j)).astype(BF16)
            local[j] = dot(b_t, x_tail)

    def begin_flows(some):
        @pl.when((pos == 0) | (pos == cut))
        def _():
            for g in some:
                for j in range(g * pairs, (g + 1) * pairs):
                    a_out[j] = local[j].astype(BF16)
                    chain(j).start()

        @pl.when(pos == cut - 1)
        def _():
            for g in some:
                for j in range(g * pairs, (g + 1) * pairs):
                    b_out[j] = local[j].astype(BF16)
                    back(j).start()

    def weigh(stage, count):
        total[...] = jnp.zeros(total.shape, F32)
        for d in range(1, count + 1):

            @pl.when(jnp.where(first, pos + d < cut, pos - d >= cut))
            def _():
                tell(d, stage).wait_recv()
                total[...] += lasts[d, stage]

    def step_a(j):
        @pl.when((pos != 0) & (pos != cut))
        def _():
            chain(j).wait_recv()

            @pl.when(pos < sp - 1)
            def _():
                a_out[j] = (a_in[j].astype(F32) * elast[j, 0:1, :] + local[j]).astype(BF16)

            @pl.when((pos != cut - 1) & (pos < sp - 1))
            def _():
                chain(j).start()

            @pl.when(pos == cut - 1)
            def _():
                cross(j).start()

    def step_b(j):
        @pl.when(pos < cut - 1)
        def _():
            back(j).wait_recv()
            b_out[j] = (b_in[j].astype(F32) + wts[j, 0:1, :] * local[j]).astype(BF16)
            back(j).start()

        @pl.when(pos >= cut)
        def _():
            carry_up(j).wait_recv()

            @pl.when(carries_up)
            def _():
                carry_up(j).start()

            @pl.when(carries_down)
            def _():
                carry_down(j).start()

    def find(s, slots):
        k = jnp.int32(-1)
        for i, at in enumerate(slots):
            k = jnp.where(s == at, i, k)
        return k

    cube = pos // CUBE
    base_a = jnp.where(first, HOP * pos + cube, HOP * (pos - cut) + cube - cut // CUBE)
    lower = jnp.logical_not(first) & (pos < middle)
    upper = pos >= middle
    last_cube = (cut - 1) // CUBE
    base_b = jnp.where(
        first,
        HOP * (cut - 1 - pos) + jnp.where(pos < CUBE, BEHIND, 0) + last_cube - cube,
        jnp.where(
            lower,
            HOP * pos + cube,
            HOP * (cut + sp - 1 - pos) + last_cube + 1 + (sp - 1) // CUBE - cube,
        ),
    )
    slots_a = [
        base_a
        + jnp.where(
            first, UP_SLOTS[k], jnp.where(pos > cut + 1, LATE_SLOTS[k], BACK_SLOTS[k])
        )
        for k in range(groups)
    ]
    slots_b = [
        base_b + jnp.where(lower, UP_SLOTS[k], BACK_SLOTS[k]) for k in range(groups)
    ]

    def flows(s):
        k_a = find(s, slots_a)

        @pl.when(k_a >= 0)
        def _():
            g = jnp.where(first, k_a, back_group(k_a))
            for p in range(pairs):
                step_a(g * pairs + p)

        k_b = find(s, slots_b)

        @pl.when(k_b >= 0)
        def _():
            g = jnp.where(lower, k_b, back_group(k_b))

            @pl.when(pos < cut - 1)
            def _():
                @pl.when(k_b < stages)
                def _():
                    weigh(k_b, cut - 1)

                weight = jnp.exp(total[...])
                for p in range(pairs):
                    j = g * pairs + p
                    moved = pltpu.roll(weight, (LANES - 2 * j) % LANES, 1)
                    wts[j, 0:1, :] = jnp.where(left_row, moved[0:1, 0:1], moved[0:1, 1:2])

            for p in range(pairs):
                step_b(g * pairs + p)

    def flow_slot(s, carry):
        flows(s)
        return carry

    def decayed():
        rate = -jnp.exp(rates[0:1, :])
        cum = steps_sum * rate
        return cum, cum[tokens - 1 : tokens, :]

    def make_states(parts, at, lines_after):
        begun, known, told = 0, set(), set()
        for number, some in enumerate(parts):
            lax.fori_loop(begun, at[number], flow_slot, 0)
            begun = at[number]
            sum_rates = rates[0:1, :]
            sources = [g * per + i for g in some for i in range(per)]
            for source in sorted(sources, key=lambda d: d < cut):
                hear(source, True)
            for g in some:
                for i in range(per):
                    source = g * per + i
                    gathered = par[source].astype(F32)
                    taps[g, 0:tap_count, i * tap_width : (i + 1) * tap_width] = gathered[
                        0:tap_count, :
                    ]
                    for part in range(3):
                        sum_rates = sum_rates + gathered[tap_count + part : tap_count + part + 1, :]
            rates[0:1, :] = sum_rates
            cum, last = decayed()
            tail = dt * jnp.exp(last - cum)
            decay = jnp.exp(last)
            for g in some:
                if g != some[0]:
                    lax.fori_loop(begun, begun + 1, flow_slot, 0)
                    begun += 1
                states(g, tail)
                for j in range(g * pairs, (g + 1) * pairs):
                    elast[j, 0:1, :] = jnp.where(
                        left_row, decay[:, 2 * j : 2 * j + 1], decay[:, 2 * j + 1 : 2 * j + 2]
                    )
                begin_flows([g])
            known |= set(some)
            for i, needed in enumerate(back_stages):
                if i not in told and set(needed) <= known:
                    told.add(i)
                    lasts[0, i] = jnp.broadcast_to(last, lasts.shape[2:])
                    for d in range(1, reach + 1):

                        @pl.when(tells(d, i))
                        def _():
                            tell(d, i).start()

            if number == lines_after:

                @pl.when(pos <= cut + 1)
                def _():
                    spread_lines()

        lax.fori_loop(begun, STATES_END, flow_slot, 0)

    def inside(g):
        for p in range(pairs):
            local_columns = slice(p * LANES, (p + 1) * LANES)
            h = g * ratio + 2 * p
            x_dt = xact[g, :, local_columns].astype(F32) * spread_columns(dt, h)
            x_low = x_dt.astype(BF16)
            parts = []
            spread = []
            for i in range(2):
                spread.append(jnp.broadcast_to(cum[:, h + i : h + i + 1], (tokens, LANES)))
                gap = spread[i] - cum_t[h + i : h + i + 1, :]
                weight = scores[g] * jnp.exp(jnp.where(causal, gap, -jnp.inf))
                parts.append(dot(weight.astype(BF16), x_low))
            inner[g, :, local_columns] = jnp.where(left_half, parts[0], parts[1])
            ecum[g, :, local_columns] = jnp.exp(jnp.where(left_half, spread[0], spread[1]))

    for source in range(3, cut):
        hear(source, early(source))

    @pl.when(pos > cut + 1)
    def _():
        spread_lines()

    near = (2 * cut) // 3

    @pl.when(pos < near)
    def _():
        make_states(up_stages, UP_STATES, min(2, stages - 1))

    @pl.when(pos >= near)
    def _():
        make_states(back_stages, BACK_STATES, min(3, stages - 1))

    cum, _ = decayed()
    cum_t = jnp.transpose(cum)

    @pl.when(first)
    def _():
        lax.fori_loop(STATES_END, FINISH, flow_slot, 0)

    @pl.when(jnp.logical_not(first))
    def _():
        for part in range(4):
            for g in range(part * groups // 4, (part + 1) * groups // 4):
                inside(g)
            begun = STATES_END + 2 * part
            lax.fori_loop(begun, begun + 2, flow_slot, 0)


    sum_down = lax.broadcasted_iota(jnp.int32, (group_width, group_width), 0) // HEAD_DIM
    sum_across = lax.broadcasted_iota(jnp.int32, (group_width, group_width), 1) // HEAD_DIM
    averager = jnp.where(sum_down == sum_across, 1.0 / HEAD_DIM, 0.0).astype(BF16)

    def finish(g):
        entering = []
        for p in range(pairs):
            j = g * pairs + p
            more = jnp.where(first, 0.0, wts[j, 0:1, :] * b_in[j].astype(F32))
            entering.append((a_in[j].astype(F32) + more).astype(BF16))
        carried = dot(cact[g], jnp.concatenate(entering, axis=1))
        core_out = (inner[g] + ecum[g] * carried).astype(BF16)
        value = core_out.astype(F32) * zs[g]
        square = value * value
        high = square.astype(BF16)
        low = (square - high.astype(F32)).astype(BF16)
        mean = dot(high, averager) + dot(low, averager)
        gain = gain_ref[0:1, pl.ds(pl.multiple_of(g * group_width, group_width), group_width)]
        normed[g] = (value * lax.rsqrt(mean + NORM_EPS) * gain).astype(BF16)

    slots_f = []
    for k in range(groups):
        both = jnp.maximum(slots_a[k], slots_b[k])
        after = jnp.maximum(slots_a[-1] + 1 + k, slots_b[k])
        needed = jnp.where(lower, after, both)
        slots_f.append(jnp.maximum(needed, FINISH + k))
    later = jnp.where(first, 0, LATER)
    ends = [jnp.where(first, 0, slots_f[-1]), slots_a[-1], slots_b[-1], RELAYS[side - 1] + later + 2]
    end = ends[0]
    for other in ends[1:]:
        end = jnp.maximum(end, other)

    def slot(s, carry):
        flows(s)
        for step, at in enumerate(RELAYS[:side]):

            @pl.when(s == at + later)
            def _():
                pass_rows(step)

        @pl.when(s == RELAYS[side - 1] + later + 2)
        def _():
            for axis in range(2):
                for i in steps:
                    for k in range(side):
                        stage_two(axis, k, i).wait_send()
                for k in range(side):
                    for i in range(side):
                        if k or i:
                            relay(axis, k, i).wait_send()

        @pl.when(jnp.logical_not(first) & (s == slots_f[0]))
        def _():
            weigh(stages - 1, reach)
            spread_rows(wts, jnp.exp(total[0:1, :]))

        k_f = find(s, slots_f)

        @pl.when(jnp.logical_not(first) & (k_f >= 0))
        def _():
            finish(jnp.where(upper, back_group(k_f), k_f))

        return carry

    for j in range(1, sp):
        share((pos + j) % sp).wait_send()

    @pl.when(pos < sp - 1)
    def _():
        for copy in halos:
            copy.wait_send()

    for i in range(stages):
        for d in range(1, reach + 1):

            @pl.when(tells(d, i))
            def _():
                tell(d, i).wait_send()

    own.wait_send()
    for axis in range(2):
        for i in steps:
            stage_one(axis, i).wait_send()

    lax.fori_loop(FINISH, end + 1, slot, 0)

    @pl.when(first)
    def _():
        for g in range(groups):
            inside(g)
            finish(g)

    own.wait_recv()
    for axis in range(2):
        for k in range(side):
            for i in range(side):
                if k or i:
                    relay(axis, k, i).wait_recv()
    blocks = out_send.shape[0]
    width = out_v.shape[1] // blocks
    outs = []
    for block in range(blocks):
        columns = slice(block * width, (block + 1) * width)
        result = dot(normed[0], w_all[0:group_width, columns])
        for g in range(1, groups):
            result += dot(normed[g], w_all[g * group_width : (g + 1) * group_width, columns])
        out_v[:, columns] = result.astype(BF16)
        copy = pltpu.make_async_copy(
            out_v.at[:, columns], out_hbm.at[0, :, columns], out_send.at[block]
        )
        copy.start()
        outs.append(copy)

    @pl.when(pos < sp - 1)
    def _():
        for j in range(chunks):
            chain(j).wait_send()

    @pl.when(first | carries_up | carries_down)
    def _():
        for j in range(chunks):
            back(j).wait_send()

    for copy in outs:
        copy.wait()


def body(
    sp,
    dp,
    stream_x,
    stream_b,
    stream_c,
    gate_z,
    step_raw,
    conv_x,
    conv_b,
    conv_c,
    decay_log,
    norm_gain,
    w_out,
):
    tokens, width = stream_x.shape[1:]
    state_width = stream_b.shape[2]
    groups = state_width // STATE
    group_width = width // groups
    chunks = width // LANES
    stages = min(4, groups - 1) + 1
    columns = w_out.shape[1]
    side = math.isqrt(dp // 2)
    anywhere = pl.BlockSpec(memory_space=pl.ANY)
    dma = pltpu.SemaphoreType.DMA
    return pl.pallas_call(
        functools.partial(kernel, sp, dp),
        out_shape=jax.ShapeDtypeStruct((1, tokens, columns), BF16),
        in_specs=[anywhere] * 11,
        out_specs=anywhere,
        scratch_shapes=[
            pltpu.VMEM((step_raw.shape[2], tokens), BF16),
            pltpu.VMEM((1, decay_log.shape[0]), F32),
            pltpu.VMEM(conv_x.shape, BF16),
            pltpu.VMEM(conv_b.shape, BF16),
            pltpu.VMEM(conv_c.shape, BF16),
            pltpu.VMEM((1, width), F32),
            pltpu.VMEM((tokens, width), BF16),
            pltpu.VMEM((tokens, state_width), BF16),
            pltpu.VMEM((tokens, state_width), BF16),
            pltpu.VMEM((tokens, width), BF16),
            pltpu.VMEM((HALO, width), BF16),
            pltpu.VMEM((HALO, state_width), BF16),
            pltpu.VMEM((HALO, state_width), BF16),
            pltpu.VMEM((sp, 8, LANES), BF16),
            pltpu.VMEM((8, LANES), F32),
            pltpu.VMEM((groups, 8, group_width + 2 * STATE), F32),
            pltpu.VMEM((LANES, tokens), F32),
            pltpu.VMEM((groups, tokens + 8, group_width + 2 * STATE), F32),
            pltpu.VMEM((groups, tokens, group_width), F32),
            pltpu.VMEM((groups, tokens, tokens), F32),
            pltpu.VMEM((groups, STATE, tokens), BF16),
            pltpu.VMEM((groups, tokens, group_width), BF16),
            pltpu.VMEM((groups, tokens, group_width), F32),
            pltpu.VMEM((groups, tokens, group_width), F32),
            pltpu.VMEM((chunks, 8, LANES), F32),
            pltpu.VMEM((chunks, 8, LANES), F32),
            pltpu.VMEM((sp, stages, 8, LANES), F32),
            pltpu.VMEM((8, LANES), F32),
            pltpu.VMEM((8, LANES), F32),
            pltpu.VMEM((groups, tokens, STATE), BF16),
            pltpu.VMEM((chunks, STATE, LANES), F32),
            pltpu.VMEM((chunks, STATE, LANES), BF16),
            pltpu.VMEM((chunks, STATE, LANES), BF16),
            pltpu.VMEM((chunks, STATE, LANES), BF16),
            pltpu.VMEM((chunks, STATE, LANES), BF16),
            pltpu.VMEM((groups, tokens, group_width), BF16),
            pltpu.VMEM((width, columns), BF16),
            dma((11,)),
            dma((sp,)),
            dma((sp,)),
            dma((sp, stages)),
            dma((sp, stages)),
            dma((3,)),
            dma((3,)),
            dma((chunks,)),
            dma((chunks,)),
            dma((chunks,)),
            dma((chunks,)),
            dma((2,)),
            dma((2, side)),
            dma((2, side)),
            dma((2, side, side)),
            dma((2, side, side)),
            dma((2, side, side)),
            dma((2, side, side)),
            pltpu.VMEM((tokens, columns), BF16),
            dma((2,)),
        ],
        compiler_params=pltpu.CompilerParams(
            collective_id=0, has_side_effects=True, vmem_limit_bytes=60 * 1024 * 1024
        ),
    )(
        stream_x,
        stream_b,
        stream_c,
        gate_z,
        jnp.swapaxes(step_raw, 1, 2),
        conv_x,
        conv_b,
        conv_c,
        decay_log.reshape(1, -1),
        norm_gain.reshape(1, -1),
        w_out,
    )


def solution(mesh):
    placed = (
        P("dp", "sp", None),
        P("dp", "sp", None),
        P("dp", "sp", None),
        P("dp", "sp", None),
        P("dp", "sp", None),
        P(None, "sp"),
        P(),
        P(),
        P("sp"),
        P(),
        P("dp", None),
    )
    return jax.shard_map(
        functools.partial(body, mesh.shape["sp"], mesh.shape["dp"]),
        mesh=mesh,
        in_specs=placed,
        out_specs=P("dp", "sp", None),
        check_vma=False,
    )
```

```python
import functools
import math

import jax
import jax.numpy as jnp
from jax import lax
from jax.experimental import pallas as pl
from jax.experimental.pallas import tpu as pltpu
from jax.sharding import PartitionSpec as P

HEAD_DIM = 64
STATE = 128
NORM_EPS = 1.0
HALO = 8
LANES = 128
HOP = 4
UP_SLOTS = (5, 7, 11, 16, 21, 23, 24, 26)
BACK_SLOTS = (13, 16, 18, 20, 23, 25, 26, 28)
UP_STATES = (2, 6, 11, 15, 19)
BACK_STATES = (12, 14, 15, 16, 20)
STATES_END = 23
FINISH = 31
RELAYS = (31, 34, 39, 45)
LATER = 7
LATE_SLOTS = (19, 20, 21, 22, 23, 25, 26, 28)
BEHIND = 4
CUBE = 4
F32 = jnp.float32
BF16 = jnp.bfloat16


def dot(a, b, precision=None):
    return jnp.dot(a, b, preferred_element_type=F32, precision=precision)


def silu(v):
    return v / (1.0 + jnp.exp(-v))


def kernel(
    sp,
    dp,
    x_hbm,
    b_hbm,
    c_hbm,
    z_hbm,
    raw_hbm,
    cx_hbm,
    cb_hbm,
    cc_hbm,
    dl_hbm,
    gain_hbm,
    w_hbm,
    out_hbm,
    raw_ref,
    dl_ref,
    cx_ref,
    cb_ref,
    cc_ref,
    gain_ref,
    x_v,
    b_v,
    c_v,
    z_v,
    halo_x,
    halo_b,
    halo_c,
    par,
    tile,
    taps,
    wide_raw,
    ext,
    zs,
    scores,
    b_ts,
    xact,
    inner,
    ecum,
    elast,
    wts,
    lasts,
    total,
    rates,
    cact,
    local,
    a_in,
    a_out,
    b_in,
    b_out,
    normed,
    w_all,
    in_sem,
    par_send,
    par_recv,
    last_send,
    last_recv,
    halo_send,
    halo_recv,
    a_send,
    a_recv,
    b_send,
    b_recv,
    own_sem,
    one_send,
    one_recv,
    two_send,
    two_recv,
    relay_send,
    relay_recv,
    out_v,
    out_send,
):
    tokens, inner_width = x_v.shape
    groups = b_v.shape[1] // STATE
    group_width = inner_width // groups
    pairs = group_width // LANES
    chunks = groups * pairs
    ratio = group_width // HEAD_DIM
    heads, local_heads = raw_ref.shape[0], dl_ref.shape[1]
    tap_count, tap_width = cx_ref.shape
    rows = w_hbm.shape[0]
    half_rows = rows // 2
    side = math.isqrt(dp // 2)
    cut = max(2, (3 * sp) // 8)
    middle = cut + (sp - cut + 1) // 2 + (1 if sp > 8 else 0)
    reach = max(cut, sp - cut) - 1

    pos = lax.axis_index("sp")
    me = lax.axis_index("dp")
    core = me % 2
    partner = me + 1 - 2 * core
    place = me // 2
    column, line = place % side, place // side
    following = (pos + 1) % sp
    preceding = (pos + sp - 1) % sp
    first = pos < cut

    def remote(src, dst, send, recv, target):
        return pltpu.make_async_remote_copy(
            src_ref=src,
            dst_ref=dst,
            send_sem=send,
            recv_sem=recv,
            device_id=target,
            device_id_type=pl.DeviceIdType.MESH,
        )

    def chip(axis, along, across):
        dx, dy = (along, across) if axis == 0 else (across, along)
        return ((line + dy + side) % side) * side + (column + dx + side) % side

    barrier = pltpu.get_barrier_semaphore()
    for j in range(1, sp):

        @pl.when(pos + j < sp)
        def _():
            pl.semaphore_signal(
                barrier,
                inc=1,
                device_id={"sp": (pos + j) % sp},
                device_id_type=pl.DeviceIdType.MESH,
            )

    @pl.when(pos > 0)
    def _():
        pl.semaphore_signal(
            barrier, inc=1, device_id={"sp": preceding}, device_id_type=pl.DeviceIdType.MESH
        )

    greeted = [{"dp": partner}]
    for axis in range(2):
        for i in range(1, side):
            greeted.append({"dp": 2 * chip(axis, i, 0) + core})
    for target in greeted:
        pl.semaphore_signal(
            barrier, inc=1, device_id=target, device_id_type=pl.DeviceIdType.MESH
        )

    sources = (
        (cx_hbm, cx_ref),
        (dl_hbm, dl_ref),
        (raw_hbm.at[0], raw_ref),
        (b_hbm.at[0], b_v),
        (c_hbm.at[0], c_v),
        (x_hbm.at[0], x_v),
        (cb_hbm, cb_ref),
        (cc_hbm, cc_ref),
        (z_hbm.at[0], z_v),
        (gain_hbm, gain_ref),
    )
    loads = [
        pltpu.make_async_copy(src, dst, in_sem.at[i]) for i, (src, dst) in enumerate(sources)
    ]
    for load in loads:
        load.start()

    def piece(axis, along, across):
        origin = 2 * chip(axis, along, across) + core
        start = pl.multiple_of(origin * rows + axis * half_rows, half_rows)
        return w_all.at[pl.ds(start, half_rows), :]

    own_rows = w_all.at[pl.ds(pl.multiple_of(me * rows, rows), rows), :]
    keep = pltpu.make_async_copy(w_hbm, own_rows, in_sem.at[len(sources)])
    keep.start()

    wide_raw[...] = jnp.zeros(wide_raw.shape, F32)
    for load in loads[0:3]:
        load.wait()
    wide_raw[0:1, 0:local_heads] = dl_ref[...]
    decays = pltpu.roll(wide_raw[0:8, :], pos * local_heads, 1)[0:1, :]
    tile[...] = jnp.zeros(tile.shape, F32)
    tile[0:tap_count, :] = cx_ref[...].astype(F32)
    for i in range(3):
        part = decays.astype(BF16).astype(F32)
        tile[tap_count + i : tap_count + i + 1, :] = part
        decays = decays - part
    par[pos] = tile[...].astype(BF16)
    wide_raw[0:heads, :] = raw_ref[...].astype(F32)
    for load in loads[3:]:
        load.wait()
    keep.wait()
    pl.semaphore_wait(barrier, len(greeted) + jnp.minimum(pos + 1, sp - 1))

    halos = [
        remote(
            src.at[pl.ds(tokens - HALO, HALO), :],
            dst,
            halo_send.at[i],
            halo_recv.at[i],
            {"sp": following},
        )
        for i, (src, dst) in enumerate(((x_v, halo_x), (b_v, halo_b), (c_v, halo_c)))
    ]

    @pl.when(pos < sp - 1)
    def _():
        for copy in halos:
            copy.start()

    def share(target):
        return remote(
            par.at[pos], par.at[pos], par_send.at[0], par_recv.at[pos], {"sp": target}
        )

    for j in range(1, sp):

        @pl.when(pos >= j)
        def _():
            share((pos + sp - j) % sp).start()

    @pl.when(pos < sp - 1)
    def _():
        share(following).start()

    def early(source):
        return (pos > 0) & (pos + 1 < source) & (source < cut)

    def hear(source, now):
        if not isinstance(now, bool):
            now = now & (pos != source)
        else:
            now = (pos != source) & jnp.logical_not(early(source))

        @pl.when(now)
        def _():
            remote(
                par.at[source],
                par.at[source],
                par_send.at[0],
                par_recv.at[source],
                {"sp": source},
            ).wait_recv()

        @pl.when(now & (pos + 1 < source))
        def _():
            share(source).start()

    def stage_one(axis, i):
        return remote(
            piece(axis, 0, 0),
            piece(axis, 0, 0),
            one_send.at[0],
            one_recv.at[axis, i - 1],
            {"dp": 2 * chip(axis, i, 0) + core},
        )

    def stage_two(axis, k, i):
        return remote(
            piece(axis, -k, 0),
            piece(axis, -k, 0),
            two_send.at[0],
            two_recv.at[axis, k, i - 1],
            {"dp": 2 * chip(axis, 0, i) + core},
        )

    def relay(axis, k, i):
        return remote(
            piece(axis, -k, -i),
            piece(axis, -k, -i),
            relay_send.at[0],
            relay_recv.at[0],
            {"dp": partner},
        )

    steps = sorted(range(1, side), key=lambda i: min(i, side - i))
    for i in steps:
        for axis in range(2):
            stage_one(axis, i).start()
    for i in steps:
        for axis in range(2):
            stage_two(axis, 0, i).start()
    own = remote(own_rows, own_rows, own_sem.at[0], own_sem.at[1], {"dp": partner})
    own.start()

    def spread_lines():
        for k in steps:
            for axis in range(2):
                stage_one(axis, k).wait_recv()
                for i in steps:
                    stage_two(axis, k, i).start()

    def pass_rows(step):
        if step == 0:
            for k in steps:
                for axis in range(2):
                    relay(axis, k, 0).start()
            which = 0
        else:
            which = steps[step - 1]
        for i in steps:
            for axis in range(2):
                stage_two(axis, which, i).wait_recv()
                relay(axis, which, i).start()

    raw = jnp.transpose(wide_raw[...])
    dt = jnp.maximum(raw, 0.0) + jnp.log(1.0 + jnp.exp(-jnp.abs(raw)))
    down = lax.broadcasted_iota(jnp.int32, (tokens, tokens), 0)
    across_tokens = lax.broadcasted_iota(jnp.int32, (tokens, tokens), 1)
    causal = down >= across_tokens
    left_half = lax.broadcasted_iota(jnp.int32, (tokens, LANES), 1) < HEAD_DIM
    left_row = left_half[0:1, :]
    for g in range(groups):
        taps[g, 0:tap_count, group_width : group_width + STATE] = cb_ref[
            :, g * STATE : (g + 1) * STATE
        ].astype(F32)
        taps[g, 0:tap_count, group_width + STATE : group_width + 2 * STATE] = cc_ref[
            :, g * STATE : (g + 1) * STATE
        ].astype(F32)
        zs[g] = silu(z_v[:, g * group_width : (g + 1) * group_width].astype(F32))

    @pl.when(pos == 0)
    def _():
        ext[:, 0:8, :] = jnp.zeros((groups, 8, ext.shape[2]), F32)

    causal_ones = jnp.where(causal, 1.0, 0.0).astype(F32)
    steps_sum = dot(causal_ones, dt, lax.Precision.HIGHEST)
    rates[...] = jnp.zeros(rates.shape, F32)

    @pl.when((pos == 0) | (pos == cut))
    def _():
        a_in[...] = jnp.zeros(a_in.shape, BF16)

    @pl.when(pos > 0)
    def _():
        for copy in halos:
            copy.wait_recv()
        for g in range(groups):
            wide = slice(g * group_width, (g + 1) * group_width)
            thin = slice(g * STATE, (g + 1) * STATE)
            ext[g, 0:8, 0:group_width] = halo_x[:, wide].astype(F32)
            ext[g, 0:8, group_width : group_width + STATE] = halo_b[:, thin].astype(F32)
            ext[g, 0:8, group_width + STATE :] = halo_c[:, thin].astype(F32)

    def conv(g, source, at):
        columns = slice(at, at + LANES)
        ext[g, 8 : 8 + tokens, columns] = source.astype(F32)
        summed = taps[g, 0:1, columns] * ext[g, 9 - tap_count : 9 - tap_count + tokens, columns]
        for k in range(1, tap_count):
            start = 9 - tap_count + k
            summed = summed + taps[g, k : k + 1, columns] * ext[g, start : start + tokens, columns]
        return silu(summed).astype(BF16)

    for g in range(groups):
        thin = slice(g * STATE, (g + 1) * STATE)
        b_act = conv(g, b_v[:, thin], group_width)
        c_act = conv(g, c_v[:, thin], group_width + STATE)
        cact[g] = c_act
        b_t = jnp.transpose(b_act)
        b_ts[g] = b_t
        scores[g] = dot(c_act, b_t)

    def ranked(center):
        near = lambda g: abs((g + 0.5) * per - center)
        return sorted(range(groups), key=near)

    def staged(order):
        single = min(4, groups - 1)
        return [[g] for g in order[:single]] + [order[single:]]

    per = group_width // tap_width
    back_order = ranked(cut + 1.2)
    up_stages, back_stages = staged(list(range(groups))), staged(back_order)
    stages = len(up_stages)

    def back_group(k):
        g = jnp.int32(back_order[0])
        for i in range(1, groups):
            g = jnp.where(k == i, back_order[i], g)
        return g

    def tell(d, i):
        target = jnp.where(first, pos + sp - d, pos + d) % sp
        return remote(
            lasts.at[0, i], lasts.at[d, i], last_send.at[d - 1, i], last_recv.at[d - 1, i], {"sp": target}
        )

    def tells(d, i):
        later = jnp.logical_not(first) & (pos + d < sp)
        return (first & (pos >= d)) | (later if i == stages - 1 else False)

    def chain(j):
        return remote(a_out.at[j], a_in.at[j], a_send.at[0], a_recv.at[j], {"sp": following})

    def cross(j):
        return remote(a_out.at[j], b_in.at[j], a_send.at[0], b_recv.at[j], {"sp": following})

    def back(j):
        return remote(b_out.at[j], b_in.at[j], b_send.at[0], b_recv.at[j], {"sp": preceding})

    def carry_up(j):
        return remote(b_in.at[j], b_in.at[j], b_send.at[0], b_recv.at[j], {"sp": following})

    def carry_down(j):
        return remote(b_in.at[j], b_in.at[j], b_send.at[0], b_recv.at[j], {"sp": preceding})

    carries_up = (pos >= cut) & (pos < middle - 1)
    carries_down = pos > middle

    def spread_rows(rows_ref, values):
        for j in range(chunks):
            rows_ref[j, 0:1, :] = jnp.where(
                left_row, values[:, 2 * j : 2 * j + 1], values[:, 2 * j + 1 : 2 * j + 2]
            )

    def spread_columns(values, h):
        return jnp.where(left_half, values[:, h : h + 1], values[:, h + 1 : h + 2])

    def states(g, tail):
        b_t = b_ts[g]
        for p in range(pairs):
            j = g * pairs + p
            x_act = conv(g, x_v[:, j * LANES : (j + 1) * LANES], p * LANES)
            xact[g, :, p * LANES : (p + 1) * LANES] = x_act
            x_tail = (x_act.astype(F32) * spread_columns(tail, 2 * j)).astype(BF16)
            local[j] = dot(b_t, x_tail)

    def begin_flows(some):
        @pl.when((pos == 0) | (pos == cut))
        def _():
            for g in some:
                for j in range(g * pairs, (g + 1) * pairs):
                    a_out[j] = local[j].astype(BF16)
                    chain(j).start()

        @pl.when(pos == cut - 1)
        def _():
            for g in some:
                for j in range(g * pairs, (g + 1) * pairs):
                    b_out[j] = local[j].astype(BF16)
                    back(j).start()

    def weigh(stage, count):
        total[...] = jnp.zeros(total.shape, F32)
        for d in range(1, count + 1):

            @pl.when(jnp.where(first, pos + d < cut, pos - d >= cut))
            def _():
                tell(d, stage).wait_recv()
                total[...] += lasts[d, stage]

    def step_a(j):
        @pl.when((pos != 0) & (pos != cut))
        def _():
            chain(j).wait_recv()

            @pl.when(pos < sp - 1)
            def _():
                a_out[j] = (a_in[j].astype(F32) * elast[j, 0:1, :] + local[j]).astype(BF16)

            @pl.when((pos != cut - 1) & (pos < sp - 1))
            def _():
                chain(j).start()

            @pl.when(pos == cut - 1)
            def _():
                cross(j).start()

    def step_b(j):
        @pl.when(pos < cut - 1)
        def _():
            back(j).wait_recv()
            b_out[j] = (b_in[j].astype(F32) + wts[j, 0:1, :] * local[j]).astype(BF16)
            back(j).start()

        @pl.when(pos >= cut)
        def _():
            carry_up(j).wait_recv()

            @pl.when(carries_up)
            def _():
                carry_up(j).start()

            @pl.when(carries_down)
            def _():
                carry_down(j).start()

    def find(s, slots):
        k = jnp.int32(-1)
        for i, at in enumerate(slots):
            k = jnp.where(s == at, i, k)
        return k

    cube = pos // CUBE
    base_a = jnp.where(first, HOP * pos + cube, HOP * (pos - cut) + cube - cut // CUBE)
    lower = jnp.logical_not(first) & (pos < middle)
    upper = pos >= middle
    last_cube = (cut - 1) // CUBE
    base_b = jnp.where(
        first,
        HOP * (cut - 1 - pos) + jnp.where(pos < CUBE, BEHIND, 0) + last_cube - cube,
        jnp.where(
            lower,
            HOP * pos + cube,
            HOP * (cut + sp - 1 - pos) + last_cube + 1 + (sp - 1) // CUBE - cube,
        ),
    )
    slots_a = [
        base_a
        + jnp.where(
            first, UP_SLOTS[k], jnp.where(pos > cut + 1, LATE_SLOTS[k], BACK_SLOTS[k])
        )
        for k in range(groups)
    ]
    slots_b = [
        base_b + jnp.where(lower, UP_SLOTS[k], BACK_SLOTS[k]) for k in range(groups)
    ]

    def flows(s):
        k_a = find(s, slots_a)

        @pl.when(k_a >= 0)
        def _():
            g = jnp.where(first, k_a, back_group(k_a))
            for p in range(pairs):
                step_a(g * pairs + p)

        k_b = find(s, slots_b)

        @pl.when(k_b >= 0)
        def _():
            g = jnp.where(lower, k_b, back_group(k_b))

            @pl.when(pos < cut - 1)
            def _():
                @pl.when(k_b < stages)
                def _():
                    weigh(k_b, cut - 1)

                weight = jnp.exp(total[...])
                for p in range(pairs):
                    j = g * pairs + p
                    moved = pltpu.roll(weight, (LANES - 2 * j) % LANES, 1)
                    wts[j, 0:1, :] = jnp.where(left_row, moved[0:1, 0:1], moved[0:1, 1:2])

            for p in range(pairs):
                step_b(g * pairs + p)

    def flow_slot(s, carry):
        flows(s)
        return carry

    def decayed():
        rate = -jnp.exp(rates[0:1, :])
        cum = steps_sum * rate
        return cum, cum[tokens - 1 : tokens, :]

    def make_states(parts, at, lines_after):
        begun, known, told = 0, set(), set()
        for number, some in enumerate(parts):
            lax.fori_loop(begun, at[number], flow_slot, 0)
            begun = at[number]
            sum_rates = rates[0:1, :]
            sources = [g * per + i for g in some for i in range(per)]
            for source in sorted(sources, key=lambda d: d < cut):
                hear(source, True)
            for g in some:
                for i in range(per):
                    source = g * per + i
                    gathered = par[source].astype(F32)
                    taps[g, 0:tap_count, i * tap_width : (i + 1) * tap_width] = gathered[
                        0:tap_count, :
                    ]
                    for part in range(3):
                        sum_rates = sum_rates + gathered[tap_count + part : tap_count + part + 1, :]
            rates[0:1, :] = sum_rates
            cum, last = decayed()
            tail = dt * jnp.exp(last - cum)
            decay = jnp.exp(last)
            for g in some:
                if g != some[0]:
                    lax.fori_loop(begun, begun + 1, flow_slot, 0)
                    begun += 1
                states(g, tail)
                for j in range(g * pairs, (g + 1) * pairs):
                    elast[j, 0:1, :] = jnp.where(
                        left_row, decay[:, 2 * j : 2 * j + 1], decay[:, 2 * j + 1 : 2 * j + 2]
                    )
                begin_flows([g])
            known |= set(some)
            for i, needed in enumerate(back_stages):
                if i not in told and set(needed) <= known:
                    told.add(i)
                    lasts[0, i] = jnp.broadcast_to(last, lasts.shape[2:])
                    for d in range(1, reach + 1):

                        @pl.when(tells(d, i))
                        def _():
                            tell(d, i).start()

            if number == lines_after:

                @pl.when(pos <= cut + 1)
                def _():
                    spread_lines()

        lax.fori_loop(begun, STATES_END, flow_slot, 0)

    def inside(g):
        for p in range(pairs):
            local_columns = slice(p * LANES, (p + 1) * LANES)
            h = g * ratio + 2 * p
            x_dt = xact[g, :, local_columns].astype(F32) * spread_columns(dt, h)
            x_low = x_dt.astype(BF16)
            parts = []
            spread = []
            for i in range(2):
                spread.append(jnp.broadcast_to(cum[:, h + i : h + i + 1], (tokens, LANES)))
                gap = spread[i] - cum_t[h + i : h + i + 1, :]
                weight = scores[g] * jnp.exp(jnp.where(causal, gap, -jnp.inf))
                parts.append(dot(weight.astype(BF16), x_low))
            inner[g, :, local_columns] = jnp.where(left_half, parts[0], parts[1])
            ecum[g, :, local_columns] = jnp.exp(jnp.where(left_half, spread[0], spread[1]))

    for source in range(3, cut):
        hear(source, early(source))

    @pl.when(pos > cut + 1)
    def _():
        spread_lines()

    near = (2 * cut) // 3

    @pl.when(pos < near)
    def _():
        make_states(up_stages, UP_STATES, min(2, stages - 1))

    @pl.when(pos >= near)
    def _():
        make_states(back_stages, BACK_STATES, min(3, stages - 1))

    cum, _ = decayed()
    cum_t = jnp.transpose(cum)

    @pl.when(first)
    def _():
        lax.fori_loop(STATES_END, FINISH, flow_slot, 0)

    @pl.when(jnp.logical_not(first))
    def _():
        for part in range(4):
            for g in range(part * groups // 4, (part + 1) * groups // 4):
                inside(g)
            begun = STATES_END + 2 * part
            lax.fori_loop(begun, begun + 2, flow_slot, 0)


    sum_down = lax.broadcasted_iota(jnp.int32, (group_width, group_width), 0) // HEAD_DIM
    sum_across = lax.broadcasted_iota(jnp.int32, (group_width, group_width), 1) // HEAD_DIM
    averager = jnp.where(sum_down == sum_across, 1.0 / HEAD_DIM, 0.0).astype(BF16)

    def finish(g):
        entering = []
        for p in range(pairs):
            j = g * pairs + p
            more = jnp.where(first, 0.0, wts[j, 0:1, :] * b_in[j].astype(F32))
            entering.append((a_in[j].astype(F32) + more).astype(BF16))
        carried = dot(cact[g], jnp.concatenate(entering, axis=1))
        core_out = (inner[g] + ecum[g] * carried).astype(BF16)
        value = core_out.astype(F32) * zs[g]
        square = value * value
        high = square.astype(BF16)
        low = (square - high.astype(F32)).astype(BF16)
        mean = dot(high, averager) + dot(low, averager)
        gain = gain_ref[0:1, pl.ds(pl.multiple_of(g * group_width, group_width), group_width)]
        normed[g] = (value * lax.rsqrt(mean + NORM_EPS) * gain).astype(BF16)

    slots_f = []
    for k in range(groups):
        both = jnp.maximum(slots_a[k], slots_b[k])
        after = jnp.maximum(slots_a[-1] + 1 + k, slots_b[k])
        needed = jnp.where(lower, after, both)
        slots_f.append(jnp.maximum(needed, FINISH + k))
    later = jnp.where(first, 0, LATER)
    ends = [jnp.where(first, 0, slots_f[-1]), slots_a[-1], slots_b[-1], RELAYS[side - 1] + later + 2]
    end = ends[0]
    for other in ends[1:]:
        end = jnp.maximum(end, other)

    def slot(s, carry):
        flows(s)
        for step, at in enumerate(RELAYS[:side]):

            @pl.when(s == at + later)
            def _():
                pass_rows(step)

        @pl.when(s == RELAYS[side - 1] + later + 2)
        def _():
            if side > 1:
                many(twos, two_send.at[0], two_recv.at[0, 0, 0]).wait_send()
                many(relays, relay_send.at[0], relay_recv.at[0]).wait_send()

        @pl.when(jnp.logical_not(first) & (s == slots_f[0]))
        def _():
            weigh(stages - 1, reach)
            spread_rows(wts, jnp.exp(total[0:1, :]))

        k_f = find(s, slots_f)

        @pl.when(jnp.logical_not(first) & (k_f >= 0))
        def _():
            finish(jnp.where(upper, back_group(k_f), k_f))

        return carry

    shared = par.at[pl.ds(0, sp - 1)]
    remote(shared, shared, par_send.at[0], par_recv.at[0], {"sp": following}).wait_send()

    @pl.when(pos < sp - 1)
    def _():
        for copy in halos:
            copy.wait_send()

    for i in range(stages):
        for d in range(1, reach + 1):

            @pl.when(tells(d, i))
            def _():
                tell(d, i).wait_send()

    def many(count, send, recv):
        some = w_all.at[pl.ds(0, count * half_rows), :]
        return remote(some, some, send, recv, {"dp": partner})

    own.wait_send()
    ones, twos, relays = 2 * (side - 1), 2 * side * (side - 1), 2 * (side * side - 1)
    if side > 1:
        many(ones, one_send.at[0], one_recv.at[0, 0]).wait_send()

    lax.fori_loop(FINISH, end + 1, slot, 0)

    @pl.when(first)
    def _():
        for g in range(groups):
            inside(g)
            finish(g)

    own.wait_recv()
    if side > 1:
        many(relays, relay_send.at[0], relay_recv.at[0]).wait_recv()
    blocks = out_send.shape[0]
    width = out_v.shape[1] // blocks
    outs = []
    for block in range(blocks):
        columns = slice(block * width, (block + 1) * width)
        result = dot(normed[0], w_all[0:group_width, columns])
        for g in range(1, groups):
            result += dot(normed[g], w_all[g * group_width : (g + 1) * group_width, columns])
        out_v[:, columns] = result.astype(BF16)
        copy = pltpu.make_async_copy(
            out_v.at[:, columns], out_hbm.at[0, :, columns], out_send.at[block]
        )
        copy.start()
        outs.append(copy)

    @pl.when(pos < sp - 1)
    def _():
        remote(a_out, a_in, a_send.at[0], a_recv.at[0], {"sp": following}).wait_send()

    @pl.when(first | carries_up | carries_down)
    def _():
        remote(b_out, b_in, b_send.at[0], b_recv.at[0], {"sp": preceding}).wait_send()

    for copy in outs:
        copy.wait()


def body(
    sp,
    dp,
    stream_x,
    stream_b,
    stream_c,
    gate_z,
    step_raw,
    conv_x,
    conv_b,
    conv_c,
    decay_log,
    norm_gain,
    w_out,
):
    tokens, width = stream_x.shape[1:]
    state_width = stream_b.shape[2]
    groups = state_width // STATE
    group_width = width // groups
    chunks = width // LANES
    stages = min(4, groups - 1) + 1
    cut = max(2, (3 * sp) // 8)
    reach = max(cut, sp - cut) - 1
    columns = w_out.shape[1]
    side = math.isqrt(dp // 2)
    anywhere = pl.BlockSpec(memory_space=pl.ANY)
    dma = pltpu.SemaphoreType.DMA
    return pl.pallas_call(
        functools.partial(kernel, sp, dp),
        out_shape=jax.ShapeDtypeStruct((1, tokens, columns), BF16),
        in_specs=[anywhere] * 11,
        out_specs=anywhere,
        scratch_shapes=[
            pltpu.VMEM((step_raw.shape[2], tokens), BF16),
            pltpu.VMEM((1, decay_log.shape[0]), F32),
            pltpu.VMEM(conv_x.shape, BF16),
            pltpu.VMEM(conv_b.shape, BF16),
            pltpu.VMEM(conv_c.shape, BF16),
            pltpu.VMEM((1, width), F32),
            pltpu.VMEM((tokens, width), BF16),
            pltpu.VMEM((tokens, state_width), BF16),
            pltpu.VMEM((tokens, state_width), BF16),
            pltpu.VMEM((tokens, width), BF16),
            pltpu.VMEM((HALO, width), BF16),
            pltpu.VMEM((HALO, state_width), BF16),
            pltpu.VMEM((HALO, state_width), BF16),
            pltpu.VMEM((sp, 8, LANES), BF16),
            pltpu.VMEM((8, LANES), F32),
            pltpu.VMEM((groups, 8, group_width + 2 * STATE), F32),
            pltpu.VMEM((LANES, tokens), F32),
            pltpu.VMEM((groups, tokens + 8, group_width + 2 * STATE), F32),
            pltpu.VMEM((groups, tokens, group_width), F32),
            pltpu.VMEM((groups, tokens, tokens), F32),
            pltpu.VMEM((groups, STATE, tokens), BF16),
            pltpu.VMEM((groups, tokens, group_width), BF16),
            pltpu.VMEM((groups, tokens, group_width), F32),
            pltpu.VMEM((groups, tokens, group_width), F32),
            pltpu.VMEM((chunks, 8, LANES), F32),
            pltpu.VMEM((chunks, 8, LANES), F32),
            pltpu.VMEM((sp, stages, 8, LANES), F32),
            pltpu.VMEM((8, LANES), F32),
            pltpu.VMEM((8, LANES), F32),
            pltpu.VMEM((groups, tokens, STATE), BF16),
            pltpu.VMEM((chunks, STATE, LANES), F32),
            pltpu.VMEM((chunks, STATE, LANES), BF16),
            pltpu.VMEM((chunks, STATE, LANES), BF16),
            pltpu.VMEM((chunks, STATE, LANES), BF16),
            pltpu.VMEM((chunks, STATE, LANES), BF16),
            pltpu.VMEM((groups, tokens, group_width), BF16),
            pltpu.VMEM((width, columns), BF16),
            dma((11,)),
            dma((1,)),
            dma((sp,)),
            dma((reach, stages)),
            dma((reach, stages)),
            dma((3,)),
            dma((3,)),
            dma((1,)),
            dma((chunks,)),
            dma((1,)),
            dma((chunks,)),
            dma((2,)),
            dma((1,)),
            dma((2, max(1, side - 1))),
            dma((1,)),
            dma((2, side, max(1, side - 1))),
            dma((1,)),
            dma((1,)),
            pltpu.VMEM((tokens, columns), BF16),
            dma((2,)),
        ],
        compiler_params=pltpu.CompilerParams(
            collective_id=0, has_side_effects=True, vmem_limit_bytes=60 * 1024 * 1024
        ),
    )(
        stream_x,
        stream_b,
        stream_c,
        gate_z,
        jnp.swapaxes(step_raw, 1, 2),
        conv_x,
        conv_b,
        conv_c,
        decay_log.reshape(1, -1),
        norm_gain.reshape(1, -1),
        w_out,
    )


def solution(mesh):
    placed = (
        P("dp", "sp", None),
        P("dp", "sp", None),
        P("dp", "sp", None),
        P("dp", "sp", None),
        P("dp", "sp", None),
        P(None, "sp"),
        P(),
        P(),
        P("sp"),
        P(),
        P("dp", None),
    )
    return jax.shard_map(
        functools.partial(body, mesh.shape["sp"], mesh.shape["dp"]),
        mesh=mesh,
        in_specs=placed,
        out_specs=P("dp", "sp", None),
        check_vma=False,
    )
```

```python
import functools
import math

import jax
import jax.numpy as jnp
from jax import lax
from jax.experimental import pallas as pl
from jax.experimental.pallas import tpu as pltpu
from jax.sharding import PartitionSpec as P

HEAD_DIM = 64
STATE = 128
NORM_EPS = 1.0
HALO = 8
LANES = 128
HOP = 4
UP_SLOTS = (5, 7, 11, 16, 21, 23, 24, 26)
BACK_SLOTS = (13, 16, 18, 20, 23, 25, 26, 28)
UP_STATES = (2, 6, 11, 15, 19)
BACK_STATES = (12, 14, 15, 16, 20)
STATES_END = 23
FINISH = 31
RELAYS = (31, 34, 39, 45)
LATER = 7
LATE_SLOTS = (19, 20, 21, 22, 23, 25, 26, 28)
BEHIND = 4
CUBE = 4
F32 = jnp.float32
BF16 = jnp.bfloat16


def dot(a, b, precision=None):
    return jnp.dot(a, b, preferred_element_type=F32, precision=precision)


def silu(v):
    return v / (1.0 + jnp.exp(-v))


def kernel(
    sp,
    dp,
    x_hbm,
    b_hbm,
    c_hbm,
    z_hbm,
    raw_hbm,
    cx_hbm,
    cb_hbm,
    cc_hbm,
    dl_hbm,
    gain_hbm,
    w_hbm,
    out_hbm,
    raw_ref,
    dl_ref,
    cx_ref,
    cb_ref,
    cc_ref,
    gain_ref,
    x_v,
    b_v,
    c_v,
    z_v,
    halo_x,
    halo_b,
    halo_c,
    par,
    tile,
    taps,
    wide_raw,
    ext,
    zs,
    scores,
    b_ts,
    xact,
    inner,
    ecum,
    elast,
    wts,
    lasts,
    total,
    rates,
    cact,
    local,
    a_in,
    a_out,
    b_in,
    b_out,
    normed,
    w_all,
    in_sem,
    par_send,
    par_recv,
    last_send,
    last_recv,
    halo_send,
    halo_recv,
    a_send,
    a_recv,
    b_send,
    b_recv,
    own_sem,
    one_send,
    one_recv,
    two_send,
    two_recv,
    relay_send,
    relay_recv,
    out_v,
    out_send,
):
    tokens, inner_width = x_v.shape
    groups = b_v.shape[1] // STATE
    group_width = inner_width // groups
    pairs = group_width // LANES
    chunks = groups * pairs
    ratio = group_width // HEAD_DIM
    heads, local_heads = raw_ref.shape[0], dl_ref.shape[1]
    tap_count, tap_width = cx_ref.shape
    rows = w_hbm.shape[0]
    half_rows = rows // 2
    side = math.isqrt(dp // 2)
    cut = max(2, (3 * sp) // 8)
    middle = cut + (sp - cut + 1) // 2 + (1 if sp > 8 else 0)
    reach = max(cut, sp - cut) - 1

    pos = lax.axis_index("sp")
    me = lax.axis_index("dp")
    core = me % 2
    partner = me + 1 - 2 * core
    place = me // 2
    column, line = place % side, place // side
    following = (pos + 1) % sp
    preceding = (pos + sp - 1) % sp
    first = pos < cut

    def remote(src, dst, send, recv, target):
        return pltpu.make_async_remote_copy(
            src_ref=src,
            dst_ref=dst,
            send_sem=send,
            recv_sem=recv,
            device_id=target,
            device_id_type=pl.DeviceIdType.MESH,
        )

    def chip(axis, along, across):
        dx, dy = (along, across) if axis == 0 else (across, along)
        return ((line + dy + side) % side) * side + (column + dx + side) % side

    barrier = pltpu.get_barrier_semaphore()
    for j in range(1, sp):

        @pl.when(pos + j < sp)
        def _():
            pl.semaphore_signal(
                barrier,
                inc=1,
                device_id={"sp": (pos + j) % sp},
                device_id_type=pl.DeviceIdType.MESH,
            )

    @pl.when(pos > 0)
    def _():
        pl.semaphore_signal(
            barrier, inc=1, device_id={"sp": preceding}, device_id_type=pl.DeviceIdType.MESH
        )

    greeted = [{"dp": partner}]
    for axis in range(2):
        for i in range(1, side):
            greeted.append({"dp": 2 * chip(axis, i, 0) + core})
    for target in greeted:
        pl.semaphore_signal(
            barrier, inc=1, device_id=target, device_id_type=pl.DeviceIdType.MESH
        )

    sources = (
        (cx_hbm, cx_ref),
        (dl_hbm, dl_ref),
        (raw_hbm.at[0], raw_ref),
        (b_hbm.at[0], b_v),
        (c_hbm.at[0], c_v),
        (x_hbm.at[0], x_v),
        (cb_hbm, cb_ref),
        (cc_hbm, cc_ref),
        (z_hbm.at[0], z_v),
        (gain_hbm, gain_ref),
    )
    loads = [
        pltpu.make_async_copy(src, dst, in_sem.at[i]) for i, (src, dst) in enumerate(sources)
    ]
    for load in loads:
        load.start()

    def piece(axis, along, across):
        origin = 2 * chip(axis, along, across) + core
        start = pl.multiple_of(origin * rows + axis * half_rows, half_rows)
        return w_all.at[pl.ds(start, half_rows), :]

    own_rows = w_all.at[pl.ds(pl.multiple_of(me * rows, rows), rows), :]
    keep = pltpu.make_async_copy(w_hbm, own_rows, in_sem.at[len(sources)])
    keep.start()

    wide_raw[...] = jnp.zeros(wide_raw.shape, F32)
    for load in loads[0:3]:
        load.wait()
    wide_raw[0:1, 0:local_heads] = dl_ref[...]
    decays = pltpu.roll(wide_raw[0:8, :], pos * local_heads, 1)[0:1, :]
    tile[...] = jnp.zeros(tile.shape, F32)
    tile[0:tap_count, :] = cx_ref[...].astype(F32)
    for i in range(3):
        part = decays.astype(BF16).astype(F32)
        tile[tap_count + i : tap_count + i + 1, :] = part
        decays = decays - part
    par[pos] = tile[...].astype(BF16)
    wide_raw[0:heads, :] = raw_ref[...].astype(F32)
    for load in loads[3:]:
        load.wait()
    keep.wait()
    pl.semaphore_wait(barrier, len(greeted) + jnp.minimum(pos + 1, sp - 1))

    halos = [
        remote(
            src.at[pl.ds(tokens - HALO, HALO), :],
            dst,
            halo_send.at[i],
            halo_recv.at[i],
            {"sp": following},
        )
        for i, (src, dst) in enumerate(((x_v, halo_x), (b_v, halo_b), (c_v, halo_c)))
    ]

    @pl.when(pos < sp - 1)
    def _():
        for copy in halos:
            copy.start()

    def share(target):
        return remote(
            par.at[pos], par.at[pos], par_send.at[0], par_recv.at[pos], {"sp": target}
        )

    for j in range(1, sp):

        @pl.when(pos >= j)
        def _():
            share((pos + sp - j) % sp).start()

    @pl.when(pos < sp - 1)
    def _():
        share(following).start()

    def early(source):
        among_first = (pos > 0) & (source < cut)
        return (pos + 1 < source) & (among_first | (pos > cut + 1))

    def hear(source, now):
        if not isinstance(now, bool):
            now = now & (pos != source)
        else:
            now = (pos != source) & jnp.logical_not(early(source))

        @pl.when(now)
        def _():
            remote(
                par.at[source],
                par.at[source],
                par_send.at[0],
                par_recv.at[source],
                {"sp": source},
            ).wait_recv()

        @pl.when(now & (pos + 1 < source))
        def _():
            share(source).start()

    def stage_one(axis, i):
        return remote(
            piece(axis, 0, 0),
            piece(axis, 0, 0),
            one_send.at[0],
            one_recv.at[axis, i - 1],
            {"dp": 2 * chip(axis, i, 0) + core},
        )

    def stage_two(axis, k, i):
        return remote(
            piece(axis, -k, 0),
            piece(axis, -k, 0),
            two_send.at[0],
            two_recv.at[axis, k, i - 1],
            {"dp": 2 * chip(axis, 0, i) + core},
        )

    def relay(axis, k, i):
        return remote(
            piece(axis, -k, -i),
            piece(axis, -k, -i),
            relay_send.at[0],
            relay_recv.at[0],
            {"dp": partner},
        )

    steps = sorted(range(1, side), key=lambda i: min(i, side - i))
    for i in steps:
        for axis in range(2):
            stage_one(axis, i).start()
    for i in steps:
        for axis in range(2):
            stage_two(axis, 0, i).start()
    own = remote(own_rows, own_rows, own_sem.at[0], own_sem.at[1], {"dp": partner})
    own.start()

    def spread_lines():
        for k in steps:
            for axis in range(2):
                stage_one(axis, k).wait_recv()
                for i in steps:
                    stage_two(axis, k, i).start()

    def pass_rows(step):
        if step == 0:
            for k in steps:
                for axis in range(2):
                    relay(axis, k, 0).start()
            which = 0
        else:
            which = steps[step - 1]
        for i in steps:
            for axis in range(2):
                stage_two(axis, which, i).wait_recv()
                relay(axis, which, i).start()

    raw = jnp.transpose(wide_raw[...])
    dt = jnp.maximum(raw, 0.0) + jnp.log(1.0 + jnp.exp(-jnp.abs(raw)))
    down = lax.broadcasted_iota(jnp.int32, (tokens, tokens), 0)
    across_tokens = lax.broadcasted_iota(jnp.int32, (tokens, tokens), 1)
    causal = down >= across_tokens
    left_half = lax.broadcasted_iota(jnp.int32, (tokens, LANES), 1) < HEAD_DIM
    left_row = left_half[0:1, :]
    for g in range(groups):
        taps[g, 0:tap_count, group_width : group_width + STATE] = cb_ref[
            :, g * STATE : (g + 1) * STATE
        ].astype(F32)
        taps[g, 0:tap_count, group_width + STATE : group_width + 2 * STATE] = cc_ref[
            :, g * STATE : (g + 1) * STATE
        ].astype(F32)
        zs[g] = silu(z_v[:, g * group_width : (g + 1) * group_width].astype(F32))

    @pl.when(pos == 0)
    def _():
        ext[:, 0:8, :] = jnp.zeros((groups, 8, ext.shape[2]), F32)

    causal_ones = jnp.where(causal, 1.0, 0.0).astype(F32)
    steps_sum = dot(causal_ones, dt, lax.Precision.HIGHEST)
    rates[...] = jnp.zeros(rates.shape, F32)

    @pl.when((pos == 0) | (pos == cut))
    def _():
        a_in[...] = jnp.zeros(a_in.shape, BF16)

    @pl.when(pos > 0)
    def _():
        for copy in halos:
            copy.wait_recv()
        for g in range(groups):
            wide = slice(g * group_width, (g + 1) * group_width)
            thin = slice(g * STATE, (g + 1) * STATE)
            ext[g, 0:8, 0:group_width] = halo_x[:, wide].astype(F32)
            ext[g, 0:8, group_width : group_width + STATE] = halo_b[:, thin].astype(F32)
            ext[g, 0:8, group_width + STATE :] = halo_c[:, thin].astype(F32)

    def conv(g, source, at):
        columns = slice(at, at + LANES)
        ext[g, 8 : 8 + tokens, columns] = source.astype(F32)
        summed = taps[g, 0:1, columns] * ext[g, 9 - tap_count : 9 - tap_count + tokens, columns]
        for k in range(1, tap_count):
            start = 9 - tap_count + k
            summed = summed + taps[g, k : k + 1, columns] * ext[g, start : start + tokens, columns]
        return silu(summed).astype(BF16)

    for g in range(groups):
        thin = slice(g * STATE, (g + 1) * STATE)
        b_act = conv(g, b_v[:, thin], group_width)
        c_act = conv(g, c_v[:, thin], group_width + STATE)
        cact[g] = c_act
        b_t = jnp.transpose(b_act)
        b_ts[g] = b_t
        scores[g] = dot(c_act, b_t)

    def ranked(center):
        near = lambda g: abs((g + 0.5) * per - center)
        return sorted(range(groups), key=near)

    def staged(order):
        single = min(4, groups - 1)
        return [[g] for g in order[:single]] + [order[single:]]

    per = group_width // tap_width
    back_order = ranked(cut + 1.2)
    up_stages, back_stages = staged(list(range(groups))), staged(back_order)
    stages = len(up_stages)

    def back_group(k):
        g = jnp.int32(back_order[0])
        for i in range(1, groups):
            g = jnp.where(k == i, back_order[i], g)
        return g

    def tell(d, i):
        target = jnp.where(first, pos + sp - d, pos + d) % sp
        return remote(
            lasts.at[0, i], lasts.at[d, i], last_send.at[d - 1, i], last_recv.at[d - 1, i], {"sp": target}
        )

    def tells(d, i):
        later = jnp.logical_not(first) & (pos + d < sp)
        return (first & (pos >= d)) | (later if i == stages - 1 else False)

    def chain(j):
        return remote(a_out.at[j], a_in.at[j], a_send.at[0], a_recv.at[j], {"sp": following})

    def cross(j):
        return remote(a_out.at[j], b_in.at[j], a_send.at[0], b_recv.at[j], {"sp": following})

    def back(j):
        return remote(b_out.at[j], b_in.at[j], b_send.at[0], b_recv.at[j], {"sp": preceding})

    def carry_up(j):
        return remote(b_in.at[j], b_in.at[j], b_send.at[0], b_recv.at[j], {"sp": following})

    def carry_down(j):
        return remote(b_in.at[j], b_in.at[j], b_send.at[0], b_recv.at[j], {"sp": preceding})

    carries_up = (pos >= cut) & (pos < middle - 1)
    carries_down = pos > middle

    def spread_rows(rows_ref, values):
        for j in range(chunks):
            rows_ref[j, 0:1, :] = jnp.where(
                left_row, values[:, 2 * j : 2 * j + 1], values[:, 2 * j + 1 : 2 * j + 2]
            )

    def spread_columns(values, h):
        return jnp.where(left_half, values[:, h : h + 1], values[:, h + 1 : h + 2])

    def states(g, tail):
        b_t = b_ts[g]
        for p in range(pairs):
            j = g * pairs + p
            x_act = conv(g, x_v[:, j * LANES : (j + 1) * LANES], p * LANES)
            xact[g, :, p * LANES : (p + 1) * LANES] = x_act
            x_tail = (x_act.astype(F32) * spread_columns(tail, 2 * j)).astype(BF16)
            local[j] = dot(b_t, x_tail)

    def begin_flows(some):
        @pl.when((pos == 0) | (pos == cut))
        def _():
            for g in some:
                for j in range(g * pairs, (g + 1) * pairs):
                    a_out[j] = local[j].astype(BF16)
                    chain(j).start()

        @pl.when(pos == cut - 1)
        def _():
            for g in some:
                for j in range(g * pairs, (g + 1) * pairs):
                    b_out[j] = local[j].astype(BF16)
                    back(j).start()

    def weigh(stage, count):
        total[...] = jnp.zeros(total.shape, F32)
        for d in range(1, count + 1):

            @pl.when(jnp.where(first, pos + d < cut, pos - d >= cut))
            def _():
                tell(d, stage).wait_recv()
                total[...] += lasts[d, stage]

    def step_a(j):
        @pl.when((pos != 0) & (pos != cut))
        def _():
            chain(j).wait_recv()

            @pl.when(pos < sp - 1)
            def _():
                a_out[j] = (a_in[j].astype(F32) * elast[j, 0:1, :] + local[j]).astype(BF16)

            @pl.when((pos != cut - 1) & (pos < sp - 1))
            def _():
                chain(j).start()

            @pl.when(pos == cut - 1)
            def _():
                cross(j).start()

    def step_b(j):
        @pl.when(pos < cut - 1)
        def _():
            back(j).wait_recv()
            b_out[j] = (b_in[j].astype(F32) + wts[j, 0:1, :] * local[j]).astype(BF16)
            back(j).start()

        @pl.when(pos >= cut)
        def _():
            carry_up(j).wait_recv()

            @pl.when(carries_up)
            def _():
                carry_up(j).start()

            @pl.when(carries_down)
            def _():
                carry_down(j).start()

    def find(s, slots):
        k = jnp.int32(-1)
        for i, at in enumerate(slots):
            k = jnp.where(s == at, i, k)
        return k

    cube = pos // CUBE
    base_a = jnp.where(first, HOP * pos + cube, HOP * (pos - cut) + cube - cut // CUBE)
    lower = jnp.logical_not(first) & (pos < middle)
    upper = pos >= middle
    last_cube = (cut - 1) // CUBE
    base_b = jnp.where(
        first,
        HOP * (cut - 1 - pos) + jnp.where(pos < CUBE, BEHIND, 0) + last_cube - cube,
        jnp.where(
            lower,
            HOP * pos + cube,
            HOP * (cut + sp - 1 - pos) + last_cube + 1 + (sp - 1) // CUBE - cube,
        ),
    )
    after_sums = jnp.where(pos > middle, 4, 0)
    slots_a = [
        base_a
        + jnp.where(
            first, UP_SLOTS[k], jnp.where(pos > cut + 1, LATE_SLOTS[k] + after_sums, BACK_SLOTS[k])
        )
        for k in range(groups)
    ]
    slots_b = [
        base_b + jnp.where(lower, UP_SLOTS[k], BACK_SLOTS[k]) for k in range(groups)
    ]

    def flows(s):
        k_a = find(s, slots_a)

        @pl.when(k_a >= 0)
        def _():
            g = jnp.where(first, k_a, back_group(k_a))
            for p in range(pairs):
                step_a(g * pairs + p)

        k_b = find(s, slots_b)

        @pl.when(k_b >= 0)
        def _():
            g = jnp.where(lower, k_b, back_group(k_b))

            @pl.when(pos < cut - 1)
            def _():
                @pl.when(k_b < stages)
                def _():
                    weigh(k_b, cut - 1)

                weight = jnp.exp(total[...])
                for p in range(pairs):
                    j = g * pairs + p
                    moved = pltpu.roll(weight, (LANES - 2 * j) % LANES, 1)
                    wts[j, 0:1, :] = jnp.where(left_row, moved[0:1, 0:1], moved[0:1, 1:2])

            for p in range(pairs):
                step_b(g * pairs + p)

    def flow_slot(s, carry):
        flows(s)
        return carry

    def decayed():
        rate = -jnp.exp(rates[0:1, :])
        cum = steps_sum * rate
        return cum, cum[tokens - 1 : tokens, :]

    def make_states(parts, at, lines_after):
        begun, known, told = 0, set(), set()
        for number, some in enumerate(parts):
            lax.fori_loop(begun, at[number], flow_slot, 0)
            begun = at[number]
            sum_rates = rates[0:1, :]
            sources = [g * per + i for g in some for i in range(per)]
            for source in sorted(sources, key=lambda d: d < cut):
                hear(source, True)
            for g in some:
                for i in range(per):
                    source = g * per + i
                    gathered = par[source].astype(F32)
                    taps[g, 0:tap_count, i * tap_width : (i + 1) * tap_width] = gathered[
                        0:tap_count, :
                    ]
                    for part in range(3):
                        sum_rates = sum_rates + gathered[tap_count + part : tap_count + part + 1, :]
            rates[0:1, :] = sum_rates
            cum, last = decayed()
            tail = dt * jnp.exp(last - cum)
            decay = jnp.exp(last)
            for g in some:
                if g != some[0]:
                    lax.fori_loop(begun, begun + 1, flow_slot, 0)
                    begun += 1
                states(g, tail)
                for j in range(g * pairs, (g + 1) * pairs):
                    elast[j, 0:1, :] = jnp.where(
                        left_row, decay[:, 2 * j : 2 * j + 1], decay[:, 2 * j + 1 : 2 * j + 2]
                    )
                begin_flows([g])
            known |= set(some)
            for i, needed in enumerate(back_stages):
                if i not in told and set(needed) <= known:
                    told.add(i)
                    lasts[0, i] = jnp.broadcast_to(last, lasts.shape[2:])
                    for d in range(1, reach + 1):

                        @pl.when(tells(d, i))
                        def _():
                            tell(d, i).start()

            if number == lines_after:

                @pl.when(pos <= cut + 1)
                def _():
                    spread_lines()

        lax.fori_loop(begun, STATES_END, flow_slot, 0)

    def inside(g):
        for p in range(pairs):
            local_columns = slice(p * LANES, (p + 1) * LANES)
            h = g * ratio + 2 * p
            x_dt = xact[g, :, local_columns].astype(F32) * spread_columns(dt, h)
            x_low = x_dt.astype(BF16)
            parts = []
            spread = []
            for i in range(2):
                spread.append(jnp.broadcast_to(cum[:, h + i : h + i + 1], (tokens, LANES)))
                gap = spread[i] - cum_t[h + i : h + i + 1, :]
                weight = scores[g] * jnp.exp(jnp.where(causal, gap, -jnp.inf))
                parts.append(dot(weight.astype(BF16), x_low))
            inner[g, :, local_columns] = jnp.where(left_half, parts[0], parts[1])
            ecum[g, :, local_columns] = jnp.exp(jnp.where(left_half, spread[0], spread[1]))

    for source in range(3, cut):
        hear(source, early(source))

    @pl.when(pos > cut + 1)
    def _():
        spread_lines()

    for source in range(cut + 4, sp):
        hear(source, early(source))

    near = (2 * cut) // 3

    @pl.when(pos < near)
    def _():
        make_states(up_stages, UP_STATES, min(2, stages - 1))

    @pl.when(pos >= near)
    def _():
        make_states(back_stages, BACK_STATES, min(3, stages - 1))

    cum, _ = decayed()
    cum_t = jnp.transpose(cum)

    @pl.when(first)
    def _():
        lax.fori_loop(STATES_END, FINISH, flow_slot, 0)

    @pl.when(jnp.logical_not(first))
    def _():
        for part in range(4):
            for g in range(part * groups // 4, (part + 1) * groups // 4):
                inside(g)
            begun = STATES_END + 2 * part
            lax.fori_loop(begun, begun + 2, flow_slot, 0)


    sum_down = lax.broadcasted_iota(jnp.int32, (group_width, group_width), 0) // HEAD_DIM
    sum_across = lax.broadcasted_iota(jnp.int32, (group_width, group_width), 1) // HEAD_DIM
    averager = jnp.where(sum_down == sum_across, 1.0 / HEAD_DIM, 0.0).astype(BF16)

    def finish(g):
        entering = []
        for p in range(pairs):
            j = g * pairs + p
            more = jnp.where(first, 0.0, wts[j, 0:1, :] * b_in[j].astype(F32))
            entering.append((a_in[j].astype(F32) + more).astype(BF16))
        carried = dot(cact[g], jnp.concatenate(entering, axis=1))
        core_out = (inner[g] + ecum[g] * carried).astype(BF16)
        value = core_out.astype(F32) * zs[g]
        square = value * value
        high = square.astype(BF16)
        low = (square - high.astype(F32)).astype(BF16)
        mean = dot(high, averager) + dot(low, averager)
        gain = gain_ref[0:1, pl.ds(pl.multiple_of(g * group_width, group_width), group_width)]
        normed[g] = (value * lax.rsqrt(mean + NORM_EPS) * gain).astype(BF16)

    slots_f = []
    for k in range(groups):
        both = jnp.maximum(slots_a[k], slots_b[k])
        after = jnp.maximum(slots_a[-1] + 1 + k, slots_b[k])
        needed = jnp.where(lower, after, both)
        slots_f.append(jnp.maximum(needed, FINISH + k))
    later = jnp.where(first, 0, LATER)
    ends = [jnp.where(first, 0, slots_f[-1]), slots_a[-1], slots_b[-1], RELAYS[side - 1] + later + 2]
    end = ends[0]
    for other in ends[1:]:
        end = jnp.maximum(end, other)

    def slot(s, carry):
        flows(s)
        for step, at in enumerate(RELAYS[:side]):

            @pl.when(s == at + later)
            def _():
                pass_rows(step)

        @pl.when(s == RELAYS[side - 1] + later + 2)
        def _():
            if side > 1:
                many(twos, two_send.at[0], two_recv.at[0, 0, 0]).wait_send()
                many(relays, relay_send.at[0], relay_recv.at[0]).wait_send()

        @pl.when(jnp.logical_not(first) & (s == slots_f[0]))
        def _():
            weigh(stages - 1, reach)
            spread_rows(wts, jnp.exp(total[0:1, :]))

        k_f = find(s, slots_f)

        @pl.when(jnp.logical_not(first) & (k_f >= 0))
        def _():
            finish(jnp.where(upper, back_group(k_f), k_f))

        return carry

    shared = par.at[pl.ds(0, sp - 1)]
    remote(shared, shared, par_send.at[0], par_recv.at[0], {"sp": following}).wait_send()

    @pl.when(pos < sp - 1)
    def _():
        for copy in halos:
            copy.wait_send()

    for i in range(stages):
        for d in range(1, reach + 1):

            @pl.when(tells(d, i))
            def _():
                tell(d, i).wait_send()

    def many(count, send, recv):
        some = w_all.at[pl.ds(0, count * half_rows), :]
        return remote(some, some, send, recv, {"dp": partner})

    own.wait_send()
    ones, twos, relays = 2 * (side - 1), 2 * side * (side - 1), 2 * (side * side - 1)
    if side > 1:
        many(ones, one_send.at[0], one_recv.at[0, 0]).wait_send()

    lax.fori_loop(FINISH, end + 1, slot, 0)

    @pl.when(first)
    def _():
        for g in range(groups):
            inside(g)
            finish(g)

    own.wait_recv()
    if side > 1:
        many(relays, relay_send.at[0], relay_recv.at[0]).wait_recv()
    blocks = out_send.shape[0]
    width = out_v.shape[1] // blocks
    outs = []
    for block in range(blocks):
        columns = slice(block * width, (block + 1) * width)
        result = dot(normed[0], w_all[0:group_width, columns])
        for g in range(1, groups):
            result += dot(normed[g], w_all[g * group_width : (g + 1) * group_width, columns])
        out_v[:, columns] = result.astype(BF16)
        copy = pltpu.make_async_copy(
            out_v.at[:, columns], out_hbm.at[0, :, columns], out_send.at[block]
        )
        copy.start()
        outs.append(copy)

    @pl.when(pos < sp - 1)
    def _():
        remote(a_out, a_in, a_send.at[0], a_recv.at[0], {"sp": following}).wait_send()

    @pl.when(first | carries_up | carries_down)
    def _():
        remote(b_out, b_in, b_send.at[0], b_recv.at[0], {"sp": preceding}).wait_send()

    for copy in outs:
        copy.wait()


def body(
    sp,
    dp,
    stream_x,
    stream_b,
    stream_c,
    gate_z,
    step_raw,
    conv_x,
    conv_b,
    conv_c,
    decay_log,
    norm_gain,
    w_out,
):
    tokens, width = stream_x.shape[1:]
    state_width = stream_b.shape[2]
    groups = state_width // STATE
    group_width = width // groups
    chunks = width // LANES
    stages = min(4, groups - 1) + 1
    cut = max(2, (3 * sp) // 8)
    reach = max(cut, sp - cut) - 1
    columns = w_out.shape[1]
    side = math.isqrt(dp // 2)
    anywhere = pl.BlockSpec(memory_space=pl.ANY)
    dma = pltpu.SemaphoreType.DMA
    return pl.pallas_call(
        functools.partial(kernel, sp, dp),
        out_shape=jax.ShapeDtypeStruct((1, tokens, columns), BF16),
        in_specs=[anywhere] * 11,
        out_specs=anywhere,
        scratch_shapes=[
            pltpu.VMEM((step_raw.shape[2], tokens), BF16),
            pltpu.VMEM((1, decay_log.shape[0]), F32),
            pltpu.VMEM(conv_x.shape, BF16),
            pltpu.VMEM(conv_b.shape, BF16),
            pltpu.VMEM(conv_c.shape, BF16),
            pltpu.VMEM((1, width), F32),
            pltpu.VMEM((tokens, width), BF16),
            pltpu.VMEM((tokens, state_width), BF16),
            pltpu.VMEM((tokens, state_width), BF16),
            pltpu.VMEM((tokens, width), BF16),
            pltpu.VMEM((HALO, width), BF16),
            pltpu.VMEM((HALO, state_width), BF16),
            pltpu.VMEM((HALO, state_width), BF16),
            pltpu.VMEM((sp, 8, LANES), BF16),
            pltpu.VMEM((8, LANES), F32),
            pltpu.VMEM((groups, 8, group_width + 2 * STATE), F32),
            pltpu.VMEM((LANES, tokens), F32),
            pltpu.VMEM((groups, tokens + 8, group_width + 2 * STATE), F32),
            pltpu.VMEM((groups, tokens, group_width), F32),
            pltpu.VMEM((groups, tokens, tokens), F32),
            pltpu.VMEM((groups, STATE, tokens), BF16),
            pltpu.VMEM((groups, tokens, group_width), BF16),
            pltpu.VMEM((groups, tokens, group_width), F32),
            pltpu.VMEM((groups, tokens, group_width), F32),
            pltpu.VMEM((chunks, 8, LANES), F32),
            pltpu.VMEM((chunks, 8, LANES), F32),
            pltpu.VMEM((sp, stages, 8, LANES), F32),
            pltpu.VMEM((8, LANES), F32),
            pltpu.VMEM((8, LANES), F32),
            pltpu.VMEM((groups, tokens, STATE), BF16),
            pltpu.VMEM((chunks, STATE, LANES), F32),
            pltpu.VMEM((chunks, STATE, LANES), BF16),
            pltpu.VMEM((chunks, STATE, LANES), BF16),
            pltpu.VMEM((chunks, STATE, LANES), BF16),
            pltpu.VMEM((chunks, STATE, LANES), BF16),
            pltpu.VMEM((groups, tokens, group_width), BF16),
            pltpu.VMEM((width, columns), BF16),
            dma((11,)),
            dma((1,)),
            dma((sp,)),
            dma((reach, stages)),
            dma((reach, stages)),
            dma((3,)),
            dma((3,)),
            dma((1,)),
            dma((chunks,)),
            dma((1,)),
            dma((chunks,)),
            dma((2,)),
            dma((1,)),
            dma((2, max(1, side - 1))),
            dma((1,)),
            dma((2, side, max(1, side - 1))),
            dma((1,)),
            dma((1,)),
            pltpu.VMEM((tokens, columns), BF16),
            dma((2,)),
        ],
        compiler_params=pltpu.CompilerParams(
            collective_id=0, has_side_effects=True, vmem_limit_bytes=60 * 1024 * 1024
        ),
    )(
        stream_x,
        stream_b,
        stream_c,
        gate_z,
        jnp.swapaxes(step_raw, 1, 2),
        conv_x,
        conv_b,
        conv_c,
        decay_log.reshape(1, -1),
        norm_gain.reshape(1, -1),
        w_out,
    )


def solution(mesh):
    placed = (
        P("dp", "sp", None),
        P("dp", "sp", None),
        P("dp", "sp", None),
        P("dp", "sp", None),
        P("dp", "sp", None),
        P(None, "sp"),
        P(),
        P(),
        P("sp"),
        P(),
        P("dp", None),
    )
    return jax.shard_map(
        functools.partial(body, mesh.shape["sp"], mesh.shape["dp"]),
        mesh=mesh,
        in_specs=placed,
        out_specs=P("dp", "sp", None),
        check_vma=False,
    )
```
